256 devices in a mesh: gr: 2 (over z_hi), fs: 16 (over z_lo, y), tp: 8 (over x, core).
Axes of the slice: x: 4, y: 4, z: 8 (z_hi: 2, z_lo: 4; z = z_hi * 4 + z_lo), core: 2. Of those that a mesh axis runs over, the one named last changes fastest.
Arguments:
- prompt: bfloat16 [16384, 2048], P(('gr', 'fs')), may hold values from -6 to 6
- norm_gain: float32 [2048], P(('gr', 'fs')), may hold values from 0.1 to 1.9
- gate_master: float32 [32, 2048, 1024], P(None, ('gr', 'fs'), 'tp'), may hold values from -6 to 6
- up_master: float32 [32, 2048, 1024], P(None, ('gr', 'fs'), 'tp'), may hold values from -6 to 6
- down_master: float32 [32, 2048, 1024], P(None, ('gr', 'fs'), 'tp'), may hold values from -6 to 6
- routes: int32 [16384, 2], P(('gr', 'fs')), may hold values from 0 to 31, as said below
- route_weights: float32 [16384, 2], P(('gr', 'fs')), may hold values from 0.1 to 0.9
Outputs:
- gate_ready: bfloat16 [32, 2048, 1024], P('fs', None, 'tp')
- up_ready: bfloat16 [32, 2048, 1024], P('fs', None, 'tp')
- down_ready: bfloat16 [32, 2048, 1024], P('fs', None, 'tp')
- blended: bfloat16 [16384, 2048], P(('gr', 'fs'), 'tp')
The draws below stay inside these ranges and needn't reach their ends.
Inputs may be any that keep to these rules, and one draw needn't show every extreme that they name: `routes`: each row names 2 different experts of one group: expert // 8 is the group. In every aligned block of 512 rows (the tokens of one index of gr and fs) half of the rows choose one group, and no expert is named more than 64 times; in every block some expert is named exactly 64 times.
All inputs are finite; a program needn't handle non-finite values.
Results may differ from the reference program's by a relative error of at most 0.015.
Values may be sent and summed in bfloat16 or wider, within the bound.
A program may use at most 128 MiB of HBM per device.

```python
import jax
import jax.numpy as jnp
from jax import lax

D = 2048
FF = 1024
N_GROUPS = 4
PER_GROUP = 8
TOP = 2
N_EXPERTS = 32
TOK_DEV = 512
CAP = 64
TOKENS = 16384
N_TP = 8


def draw_routes(key, part):
    blocks = TOKENS // TOK_DEV
    half_block = TOK_DEV // 2
    subkeys = jax.random.split(jax.random.fold_in(key, 7), 8)
    common = jax.random.randint(subkeys[0], (), 0, N_GROUPS)
    own_big = jax.random.randint(subkeys[1], (blocks,), 0, N_GROUPS)
    big_group = jnp.where(jnp.arange(blocks) < blocks // 2, common, own_big)
    cut_points = jnp.sort(jax.random.randint(subkeys[2], (blocks, N_GROUPS - 2), 0, half_block + 1), axis=1)
    edges = jnp.concatenate([jnp.zeros((blocks, 1), jnp.int32), cut_points.astype(jnp.int32), jnp.full((blocks, 1), half_block, jnp.int32)], axis=1)
    small_sizes = edges[:, 1:] - edges[:, :-1]
    groups = jnp.arange(N_GROUPS, dtype=jnp.int32)
    offset = (groups[None, :] - big_group[:, None] - 1) % N_GROUPS
    group_sizes = jnp.where(offset == N_GROUPS - 1, half_block, jnp.take_along_axis(small_sizes, jnp.minimum(offset, N_GROUPS - 2), axis=1))
    group_ends = jnp.cumsum(group_sizes, axis=1)
    starts = group_ends - group_sizes
    token_ranks = jnp.argsort(jax.random.randint(subkeys[3], (blocks, TOK_DEV), 0, 1 << 20) * TOK_DEV + jnp.arange(TOK_DEV, dtype=jnp.int32)[None, :], axis=1)
    group_of = jnp.sum((token_ranks[:, :, None] >= group_ends[:, None, :]).astype(jnp.int32), axis=2)
    inner_rank = token_ranks - jnp.take_along_axis(starts, group_of, axis=1)
    first_shift = jax.random.randint(subkeys[4], (blocks, N_GROUPS), 0, PER_GROUP)
    second_step = jax.random.randint(subkeys[5], (blocks, N_GROUPS), 1, PER_GROUP)
    local_order = jnp.argsort(jax.random.randint(subkeys[6], (blocks, N_GROUPS, PER_GROUP), 0, 1 << 20) * PER_GROUP + jnp.arange(PER_GROUP, dtype=jnp.int32), axis=2)
    first_local = (inner_rank + jnp.take_along_axis(first_shift, group_of, axis=1)) % PER_GROUP
    second_local = (first_local + jnp.take_along_axis(second_step, group_of, axis=1)) % PER_GROUP
    group_table = local_order[jnp.arange(blocks)[:, None], group_of]
    local_pair = jnp.take_along_axis(group_table, jnp.stack([first_local, second_local], axis=2), axis=2)
    experts = group_of[:, :, None] * PER_GROUP + local_pair
    return experts.reshape(TOKENS, TOP).astype(jnp.int32)


def steps_of(own_key, extent, shards, least, largest):
    def one(dim, shards_of):
        heights = jax.random.uniform(jax.random.fold_in(jax.random.fold_in(own_key, 6), dim), (shards_of,), jnp.float32, least / len(shards), largest / len(shards))
        return jnp.repeat(jnp.exp(heights), extent[dim] // shards_of).reshape((-1,) + (1,) * (len(extent) - dim - 1))

    loudness = one(*shards[0])
    for cut in shards[1:]:
        loudness = loudness * one(*cut)
    return loudness


def gaussian(key, dims, width, reach, cuts=(), held_as=jnp.bfloat16):
    entries = jax.random.normal(key, dims, jnp.float32) * width
    if len(cuts) > 0:
        entries = steps_of(key, dims, cuts, -0.22, 0.18) * entries
    return jnp.clip(entries, min=-reach, max=reach).astype(held_as)


def setup_inputs(seed: int = 0) -> dict:
    streams_of = jax.random.split(jax.random.key(seed), 8)
    return {
        "prompt": gaussian(streams_of[0], (TOKENS, D), 1.0, 6.0, ((0, 32),)),
        "norm_gain": jnp.clip(1.0 + 0.18 * jax.random.normal(streams_of[1], (D,), jnp.float32), 0.1, 1.9),
        "gate_master": gaussian(streams_of[2], (N_EXPERTS, D, FF), 1.0, 6.0, ((1, 32), (2, 8)), jnp.float32),
        "up_master": gaussian(streams_of[3], (N_EXPERTS, D, FF), 1.0, 6.0, ((1, 32), (2, 8)), jnp.float32),
        "down_master": gaussian(streams_of[4], (N_EXPERTS, D, FF), 1.0, 6.0, ((1, 32), (2, 8)), jnp.float32),
        "routes": draw_routes(jax.random.fold_in(streams_of[7], 71), 0),
        "route_weights": jnp.clip(0.1 + 0.79999997 * jax.random.uniform(streams_of[6], (TOKENS, TOP), jnp.float32) ** steps_of(streams_of[6], (TOKENS, TOP), ((0, 32),), -0.2, 0.2), 0.1, 0.9),
    }


EPS = 1e-06

def reference(prompt, norm_gain, gate_master, up_master, down_master, routes, route_weights):
    gate_new = (norm_gain[None, :, None] * gate_master).astype(jnp.bfloat16)
    up_new = (norm_gain[None, :, None] * up_master).astype(jnp.bfloat16)
    down_new = down_master.astype(jnp.bfloat16)
    prompt_wide = prompt.astype(jnp.float32)
    normed = (prompt_wide * lax.rsqrt(lax.optimization_barrier(jnp.mean(prompt_wide * prompt_wide, axis=-1, keepdims=True)) + EPS)).astype(jnp.bfloat16)
    route_list = routes.reshape(-1).astype(jnp.int32)
    route_hits = (route_list[:, None] == jnp.arange(N_EXPERTS, dtype=jnp.int32)[None, :]).astype(jnp.int32)
    slot_rank = lax.optimization_barrier(jnp.sum((jnp.cumsum(route_hits, axis=0).astype(jnp.int32) - 1) * route_hits, axis=1)).astype(jnp.int32)
    expert_room = TOKENS // TOK_DEV * CAP
    slot_index = (route_list * expert_room + slot_rank).astype(jnp.int32)
    token_of = (jnp.arange(route_list.shape[0], dtype=jnp.int32) // TOP).astype(jnp.int32)
    slot_owner = jnp.zeros((N_EXPERTS * expert_room,), jnp.int32).at[slot_index].set(token_of)

    def expert(operands):
        row_ids, gate_rows, up_rows, down_rows = operands
        picked = normed[row_ids]
        pre_gate = jnp.dot(picked, gate_rows, preferred_element_type=jnp.float32) * D ** (-0.5)
        pre_up = jnp.dot(picked, up_rows, preferred_element_type=jnp.float32) * D ** (-0.5)
        hidden = (jax.nn.silu(pre_gate) * pre_up).astype(jnp.bfloat16)
        hidden_blocks = hidden.astype(jnp.float32).reshape(row_ids.shape[0], N_TP, FF // N_TP)
        down_blocks = down_rows.astype(jnp.float32).reshape(D, N_TP, FF // N_TP)
        partial_value = (jnp.einsum('rnf,dnf->rnd', hidden_blocks, down_blocks) * FF ** (-0.5)).astype(jnp.bfloat16)
        return lax.optimization_barrier(jnp.sum(partial_value.astype(jnp.float32), axis=1)).astype(jnp.bfloat16)
    results = lax.map(expert, (slot_owner.reshape(N_EXPERTS, expert_room), gate_new, up_new, down_new))
    per_choice = results.reshape(N_EXPERTS * expert_room, D)[slot_index].reshape(TOKENS, TOP, D)
    blended = lax.optimization_barrier(jnp.sum(per_choice.astype(jnp.float32) * route_weights[:, :, None], axis=1))
    return (gate_new, up_new, down_new, blended.astype(jnp.bfloat16))
```

```python
import jax
import jax.numpy as jnp
from jax import lax
from jax.experimental import pallas as pl
from jax.experimental.pallas import tpu as pltpu
from jax.sharding import PartitionSpec as P

MESH = pl.DeviceIdType.MESH
EPS = 1e-06
BF = jnp.bfloat16
F32 = jnp.float32

PLANES = ((0, 0, 0, 64), (1, 1, 0, 64), (2, -1, 0, 64), (3, 2, 0, 32), (3, -2, 32, 64))
TOK0, TOK1, HID0, HID1 = 0, 1, 2, 3
OWN_R, OWN_L, OWN_C, FAR_R, FAR_L, C_L, C_R, C_F0, C_F1 = range(9)


def kernel(
    prompt_hbm,
    gain_ref,
    gate_hbm,
    up_hbm,
    down_hbm,
    routes_ref,
    rw_ref,
    gate_out,
    up_out,
    down_out,
    blend_out,
    prompt_v,
    gate_v,
    up_v,
    down_v,
    stage_gu,
    stage_d,
    w_gu,
    w_d,
    slots_x,
    tok,
    hid,
    dx,
    outs,
    ans,
    s0,
    s1,
    acc,
    blend_v,
    load_sem,
    store_sem,
    wsend,
    wrecv,
    tsend,
    trecv,
    asend,
    arecv,
    dsend,
    drecv,
    rsend,
    rrecv,
):
    g = lax.axis_index("gr")
    f = lax.axis_index("fs")
    t = lax.axis_index("tp")
    me = g * 16 + f
    z = g * 4 + f // 4
    y = lax.rem(f, 4)
    x = t // 2
    c = lax.rem(t, 2)

    def at_zy(zz, yy):
        zz = lax.rem(zz + 16, 8)
        yy = lax.rem(yy + 8, 4)
        return zz // 4, lax.rem(zz, 4) * 4 + yy

    right = (g, f, lax.rem(x + 1, 4) * 2 + c)
    left = (g, f, lax.rem(x + 3, 4) * 2 + c)
    other = (g, f, x * 2 + 1 - c)
    t_l = lax.rem(x + 3, 4) * 2 + c
    t_r = lax.rem(x + 1, 4) * 2 + c
    t_f = lax.rem(x + 2, 4) * 2 + c

    loads = [
        pltpu.make_async_copy(down_hbm, down_v, load_sem.at[0]),
        pltpu.make_async_copy(prompt_hbm, prompt_v, load_sem.at[1]),
        pltpu.make_async_copy(gate_hbm, gate_v, load_sem.at[2]),
        pltpu.make_async_copy(up_hbm, up_v, load_sem.at[3]),
    ]
    for ld in loads:
        ld.start()

    barrier = pltpu.get_barrier_semaphore()

    def greet_zy(i, carry):
        gg, ff = at_zy(z + i // 4, y + lax.rem(i, 4))
        pl.semaphore_signal(barrier, inc=1, device_id=(gg, ff, t), device_id_type=MESH)
        return carry

    lax.fori_loop(1, 32, greet_zy, 0)

    def greet_tp(i, carry):
        pl.semaphore_signal(barrier, inc=1, device_id=(g, f, lax.rem(t + i, 8)), device_id_type=MESH)
        return carry

    lax.fori_loop(1, 8, greet_tp, 0)

    eye = lax.broadcasted_iota(jnp.int32, (64, 64), 0) == lax.broadcasted_iota(jnp.int32, (64, 64), 1)
    gain = jnp.sum(jnp.where(eye, gain_ref[...], 0.0), axis=1, keepdims=True)

    def round_d(p):
        def body(i, carry):
            stage_d[p, i] = down_v[i, p].astype(BF)
            return carry

        lax.fori_loop(0, 16, body, 0)
        w_d[p, me] = stage_d[p, f]

    def round_gu(p):
        def body(i, carry):
            stage_gu[p, i, :, 0:128] = (gain * gate_v[i, p]).astype(BF)
            stage_gu[p, i, :, 128:256] = (gain * up_v[i, p]).astype(BF)
            return carry

        lax.fori_loop(0, 16, body, 0)
        w_gu[p, me] = stage_gu[p, f]

    def send_w(stage, dest, p, sem):
        def body(i, carry):
            gg, ff = at_zy(z + i // 4, y + lax.rem(i, 4))
            pltpu.make_async_remote_copy(
                src_ref=stage.at[p, ff],
                dst_ref=dest.at[p, me],
                send_sem=wsend.at[sem],
                recv_sem=wrecv.at[sem],
                device_id=(gg, ff, t),
                device_id_type=MESH,
            ).start()
            return carry

        lax.fori_loop(1, 32, body, 0)

    def await_w(sems, dest, p, sem):
        part = dest.at[p, pl.ds(0, 31)]
        pltpu.make_async_copy(part, part, sems.at[sem]).wait()

    def copy_to(ref, sems, i, where):
        return pltpu.make_async_remote_copy(
            src_ref=ref,
            dst_ref=ref,
            send_sem=asend.at[sems, i],
            recv_sem=arecv.at[sems, i],
            device_id=where,
            device_id_type=MESH,
        )

    def piece(kind, tt, half):
        p = kind % 2
        if kind < 2:
            ref = tok.at[p, tt]
            return ref if half is None else ref.at[pl.ds(8 * half, 8)]
        ref = hid.at[p, tt]
        return ref if half is None else ref.at[pl.ds(512 * half, 512)]

    def ag_own(kind):
        ref = piece(kind, t, None)
        copy_to(ref, kind, OWN_R, right).start()
        copy_to(ref, kind, OWN_L, left).start()
        copy_to(ref, kind, OWN_C, other).start()

    def ag_relay(kind):
        copy_to(piece(kind, t_l, None), kind, OWN_R, right).wait_recv()
        copy_to(piece(kind, t_l, 0), kind, FAR_R, right).start()
        copy_to(piece(kind, t_l, None), kind, C_L, other).start()
        copy_to(piece(kind, t_r, None), kind, OWN_L, left).wait_recv()
        copy_to(piece(kind, t_r, 1), kind, FAR_L, left).start()
        copy_to(piece(kind, t_r, None), kind, C_R, other).start()

    def ag_far(kind):
        copy_to(piece(kind, t_f, 0), kind, FAR_R, right).wait_recv()
        copy_to(piece(kind, t_f, 0), kind, C_F0, other).start()
        copy_to(piece(kind, t_f, 1), kind, FAR_L, left).wait_recv()
        copy_to(piece(kind, t_f, 1), kind, C_F1, other).start()

    def ag_end(kind):
        for i, half in ((OWN_C, None), (C_L, None), (C_R, None), (C_F0, 0), (C_F1, 1)):
            copy_to(piece(kind, t, half), kind, i, other).wait_recv()

    def ag_drain(kind):
        for i, half in (
            (OWN_R, None),
            (OWN_L, None),
            (OWN_C, None),
            (FAR_R, 0),
            (FAR_L, 1),
            (C_L, None),
            (C_R, None),
            (C_F0, 0),
            (C_F1, 1),
        ):
            copy_to(piece(kind, t, half), kind, i, other).wait_send()

    def send_tokens(p):
        for j, dz, lo, hi in PLANES:
            for dy in range(4):
                gg, ff = at_zy(z + dz, y + dy)
                if dz == 0 and dy == 0:
                    continue
                pltpu.make_async_remote_copy(
                    src_ref=slots_x.at[p, ff, pl.ds(lo, hi - lo)],
                    dst_ref=tok.at[p, t, j * 4 + y, pl.ds(lo, hi - lo)],
                    send_sem=tsend.at[p],
                    recv_sem=trecv.at[p],
                    device_id=(gg, ff, t),
                    device_id_type=MESH,
                ).start()
        tok[p, t, y] = slots_x[p, f]

    def await_tokens(sems, p):
        part = slots_x.at[p, pl.ds(0, 15)]
        pltpu.make_async_copy(part, part, sems.at[p]).wait()

    def send_back(p):
        for j, dz, lo, hi in PLANES:
            for dy in range(4):
                if dz == 0 and dy == 0:
                    continue
                gg, ff = at_zy(z - dz, y + dy)
                pltpu.make_async_remote_copy(
                    src_ref=outs.at[p, j * 4 + lax.rem(y + dy, 4), pl.ds(lo, hi - lo)],
                    dst_ref=ans.at[p, f, pl.ds(lo, hi - lo)],
                    send_sem=rsend.at[p],
                    recv_sem=rrecv.at[p],
                    device_id=(gg, ff, t),
                    device_id_type=MESH,
                ).start()
        ans[p, f] = outs[p, y]

    def await_back(sems, p):
        part = outs.at[p, pl.ds(0, 15)]
        pltpu.make_async_copy(part, part, sems.at[p]).wait()

    def send_dx(p):
        def body(i, carry):
            tt = lax.rem(t + i, 8)
            pltpu.make_async_remote_copy(
                src_ref=w_d.at[p, pl.ds(tt * 4, 4)],
                dst_ref=dx.at[p, t],
                send_sem=dsend.at[p],
                recv_sem=drecv.at[p],
                device_id=(g, f, tt),
                device_id_type=MESH,
            ).start()
            return carry

        lax.fori_loop(1, 8, body, 0)
        dx[p, t] = w_d[p, pl.ds(t * 4, 4)]

    def await_dx(sems, p):
        part = dx.at[p, pl.ds(0, 7)]
        pltpu.make_async_copy(part, part, sems.at[p]).wait()

    def hidden(p):
        def body(r, carry):
            rows = jnp.concatenate(
                [tok[p, tt, pl.ds(r * 4, 4)].reshape(256, 256) for tt in range(8)], axis=1
            )
            pre = jnp.dot(rows, w_gu[p].reshape(2048, 256), preferred_element_type=F32) * 2048 ** (-0.5)
            gate, up = pre[:, 0:128], pre[:, 128:256]
            value = gate / (1.0 + jnp.exp(-gate)) * up
            hid[p, t, pl.ds(r * 256, 256)] = value.astype(BF)
            return carry

        lax.fori_loop(0, 4, body, 0)

    def expert_out(p):
        def body(r, carry):
            rows = jnp.concatenate([hid[p, tt, pl.ds(r * 256, 256)] for tt in range(8)], axis=1)
            cols = jnp.concatenate([dx[p, tt].reshape(256, 128) for tt in range(8)], axis=1)
            value = lax.dot_general(rows, cols, (((1,), (1,)), ((), ())), preferred_element_type=F32)
            value = (value * 1024 ** (-0.5)).astype(BF)
            outs[p, pl.ds(r * 4, 4)] = value.reshape(4, 64, 256)
            return carry

        lax.fori_loop(0, 4, body, 0)

    def blend(p):
        for r in range(2):
            rows = pl.ds(r * 256, 256)
            values = ans[p].reshape(1024, 256)
            first = jnp.dot(s0[p, rows], values, preferred_element_type=F32)
            second = jnp.dot(s1[p, rows], values, preferred_element_type=F32)
            part = rw_ref[rows, 0:1] * first + rw_ref[rows, 1:2] * second
            if p == 0:
                acc[rows] = part
            else:
                blend_v[rows] = (acc[rows] + part).astype(BF)

    loads[0].wait()
    round_d(0)
    pl.semaphore_wait(barrier, 38)
    send_w(stage_d, w_d, 0, 0)

    lanes = lax.broadcasted_iota(jnp.int32, (512, 128), 1)
    hit0 = jnp.where(routes_ref[:, 0:1] == lanes, 1.0, 0.0)
    hit1 = jnp.where(routes_ref[:, 1:2] == lanes, 1.0, 0.0)
    row_i = lax.broadcasted_iota(jnp.int32, (512, 512), 0)
    col_i = lax.broadcasted_iota(jnp.int32, (512, 512), 1)
    before = jnp.where(col_i < row_i, 1.0, 0.0).astype(BF)
    rank0 = jnp.dot(before, hit0.astype(BF), preferred_element_type=F32)
    rank1 = jnp.dot(before, hit1.astype(BF), preferred_element_type=F32) + jnp.sum(hit0, axis=0, keepdims=True)
    place = ((lanes >> 1) * 64 + (lanes & 1) * 1024).astype(F32)
    slot0 = jnp.sum((rank0 + place) * hit0, axis=1, keepdims=True)
    slot1 = jnp.sum((rank1 + place) * hit1, axis=1, keepdims=True)
    diag = col_i == row_i
    slot0_row = jnp.sum(jnp.where(diag, slot0, 0.0), axis=0, keepdims=True)
    slot1_row = jnp.sum(jnp.where(diag, slot1, 0.0), axis=0, keepdims=True)

    loads[1].wait()
    wide = prompt_v[...].astype(F32)
    scale = lax.rsqrt(jnp.sum(wide * wide, axis=1, keepdims=True) * (1.0 / 2048) + EPS)
    mine = prompt_v[:, pl.ds(pl.multiple_of(t * 256, 256), 256)].astype(F32)
    normed = (mine * scale).astype(BF)
    for p in range(2):
        for r in range(4):
            number = (lax.broadcasted_iota(jnp.int32, (256, 512), 0) + (p * 1024 + r * 256)).astype(F32)
            pick = jnp.where((number == slot0_row) | (number == slot1_row), 1.0, 0.0).astype(BF)
            rows = jnp.dot(pick, normed, preferred_element_type=F32).astype(BF)
            slots_x[p, pl.ds(r * 4, 4)] = rows.reshape(4, 64, 256)
        send_tokens(p)

    loads[2].wait()
    loads[3].wait()
    round_gu(0)
    send_w(stage_gu, w_gu, 0, 2)
    round_gu(1)
    send_w(stage_gu, w_gu, 1, 3)
    round_d(1)
    for p in range(2):
        number = (lax.broadcasted_iota(jnp.int32, (512, 1024), 1) + p * 1024).astype(F32)
        s0[p] = jnp.where(number == slot0, 1.0, 0.0).astype(BF)
        s1[p] = jnp.where(number == slot1, 1.0, 0.0).astype(BF)

    await_tokens(trecv, 0)
    ag_own(TOK0)
    await_tokens(trecv, 1)
    ag_own(TOK1)
    ag_relay(TOK0)
    ag_relay(TOK1)
    await_w(wrecv, w_d, 0, 0)
    send_dx(0)
    stores = []

    def store(src, dst, i):
        cp = pltpu.make_async_copy(src, dst, store_sem.at[i])
        cp.start()
        stores.append(cp)

    store(w_d.at[0], down_out.at[0], 0)
    ag_far(TOK0)
    ag_end(TOK0)
    await_w(wrecv, w_gu, 0, 2)
    hidden(0)
    ag_own(HID0)
    store(w_gu.at[0, :, :, pl.ds(0, 128)], gate_out.at[0], 1)
    store(w_gu.at[0, :, :, pl.ds(128, 128)], up_out.at[0], 2)
    ag_far(TOK1)
    ag_relay(HID0)
    ag_far(HID0)
    await_dx(drecv, 0)
    ag_end(HID0)
    expert_out(0)
    send_back(0)
    send_w(stage_d, w_d, 1, 1)
    ag_end(TOK1)
    await_w(wrecv, w_gu, 1, 3)
    hidden(1)
    ag_own(HID1)
    store(w_gu.at[1, :, :, pl.ds(0, 128)], gate_out.at[1], 3)
    store(w_gu.at[1, :, :, pl.ds(128, 128)], up_out.at[1], 4)
    ag_relay(HID1)
    ag_far(HID1)
    ag_end(HID1)
    await_back(rrecv, 0)
    blend(0)
    await_w(wrecv, w_d, 1, 1)
    send_dx(1)
    store(w_d.at[1], down_out.at[1], 5)
    await_dx(drecv, 1)
    expert_out(1)
    send_back(1)
    for kind in range(4):
        ag_drain(kind)
    for p in range(2):
        await_w(wsend, w_d, p, p)
        await_w(wsend, w_gu, p, 2 + p)
        await_tokens(tsend, p)
        await_dx(dsend, p)
    await_back(rsend, 0)
    await_back(rrecv, 1)
    blend(1)
    store(blend_v, blend_out, 6)
    await_back(rsend, 1)
    for cp in stores:
        cp.wait()


def per_device(prompt, norm_gain, gate_master, up_master, down_master, routes, route_weights):
    any_spec = pl.BlockSpec(memory_space=pl.ANY)
    vmem = pl.BlockSpec(memory_space=pltpu.VMEM)
    ready = jax.ShapeDtypeStruct((2, 32, 64, 128), BF)
    dma = pltpu.SemaphoreType.DMA
    split = lambda a: a.reshape(16, 2, 64, 128)
    gate, up, down, out = pl.pallas_call(
        kernel,
        out_shape=(ready, ready, ready, jax.ShapeDtypeStruct((512, 256), BF)),
        in_specs=[any_spec, vmem, any_spec, any_spec, any_spec, vmem, vmem],
        out_specs=(any_spec,) * 4,
        scratch_shapes=[
            pltpu.VMEM((512, 2048), BF),
            pltpu.VMEM((16, 2, 64, 128), F32),
            pltpu.VMEM((16, 2, 64, 128), F32),
            pltpu.VMEM((16, 2, 64, 128), F32),
            pltpu.VMEM((2, 16, 64, 256), BF),
            pltpu.VMEM((2, 16, 64, 128), BF),
            pltpu.VMEM((2, 32, 64, 256), BF),
            pltpu.VMEM((2, 32, 64, 128), BF),
            pltpu.VMEM((2, 16, 64, 256), BF),
            pltpu.VMEM((2, 8, 16, 64, 256), BF),
            pltpu.VMEM((2, 8, 1024, 128), BF),
            pltpu.VMEM((2, 8, 4, 64, 128), BF),
            pltpu.VMEM((2, 16, 64, 256), BF),
            pltpu.VMEM((2, 16, 64, 256), BF),
            pltpu.VMEM((2, 512, 1024), BF),
            pltpu.VMEM((2, 512, 1024), BF),
            pltpu.VMEM((512, 256), F32),
            pltpu.VMEM((512, 256), BF),
            dma((4,)),
            dma((7,)),
            dma((4,)),
            dma((4,)),
            dma((2,)),
            dma((2,)),
            dma((4, 9)),
            dma((4, 9)),
            dma((2,)),
            dma((2,)),
            dma((2,)),
            dma((2,)),
        ],
        compiler_params=pltpu.CompilerParams(
            collective_id=0, has_side_effects=True, vmem_limit_bytes=56 * 2**20
        ),
    )(
        prompt,
        norm_gain.reshape(1, 64),
        split(gate_master),
        split(up_master),
        split(down_master),
        routes,
        route_weights,
    )
    flat = lambda a: a.reshape(2, 2048, 128)
    return flat(gate), flat(up), flat(down), out


def solution(mesh):
    in_specs = (
        P(("gr", "fs"), None),
        P(("gr", "fs")),
        P(None, ("gr", "fs"), "tp"),
        P(None, ("gr", "fs"), "tp"),
        P(None, ("gr", "fs"), "tp"),
        P(("gr", "fs"), None),
        P(("gr", "fs"), None),
    )
    out_specs = (
        P("fs", None, "tp"),
        P("fs", None, "tp"),
        P("fs", None, "tp"),
        P(("gr", "fs"), "tp"),
    )
    return jax.shard_map(
        per_device, mesh=mesh, in_specs=in_specs, out_specs=out_specs, check_vma=False
    )
```

```python
import jax
import jax.numpy as jnp
from jax import lax
from jax.experimental import pallas as pl
from jax.experimental.pallas import tpu as pltpu
from jax.sharding import PartitionSpec as P

MESH = pl.DeviceIdType.MESH
EPS = 1e-06
BF = jnp.bfloat16
F32 = jnp.float32

PLANES = ((0, 0, 0, 64), (1, 1, 0, 64), (2, -1, 0, 64), (3, 2, 0, 32), (3, -2, 32, 64))
TOK0, TOK1, HID0, HID1 = 0, 1, 2, 3
OWN_R, OWN_L, OWN_C, FAR_R, FAR_L, C_L, C_R, C_F0, C_F1 = range(9)


def kernel(
    prompt_hbm,
    gain_hbm,
    gate_hbm,
    up_hbm,
    down_hbm,
    routes_hbm,
    rw_hbm,
    w_gu0,
    w_gu1,
    w_d,
    blend_v,
    gain_ref,
    routes_ref,
    rw_ref,
    prompt_v,
    gate_v,
    up_v,
    down_v,
    stage_gu,
    stage_d,
    slots_x,
    tok,
    hid,
    dx,
    outs,
    ans,
    s0,
    s1,
    acc,
    load_sem,
    wsend,
    wrecv,
    tsend,
    trecv,
    asend,
    arecv,
    dsend,
    drecv,
    rsend,
    rrecv,
):
    w_gu = (w_gu0, w_gu1)
    g = lax.axis_index("gr")
    f = lax.axis_index("fs")
    t = lax.axis_index("tp")
    me = g * 16 + f
    z = g * 4 + f // 4
    y = lax.rem(f, 4)
    x = t // 2
    c = lax.rem(t, 2)

    def at_zy(zz, yy):
        zz = lax.rem(zz + 16, 8)
        yy = lax.rem(yy + 8, 4)
        return zz // 4, lax.rem(zz, 4) * 4 + yy

    right = (g, f, lax.rem(x + 1, 4) * 2 + c)
    left = (g, f, lax.rem(x + 3, 4) * 2 + c)
    other = (g, f, x * 2 + 1 - c)
    t_l = lax.rem(x + 3, 4) * 2 + c
    t_r = lax.rem(x + 1, 4) * 2 + c
    t_f = lax.rem(x + 2, 4) * 2 + c

    barrier = pltpu.get_barrier_semaphore()

    def greet_zy(i, carry):
        gg, ff = at_zy(z + i // 4, y + lax.rem(i, 4))
        pl.semaphore_signal(barrier, inc=1, device_id=(gg, ff, t), device_id_type=MESH)
        return carry

    lax.fori_loop(1, 32, greet_zy, 0)

    def greet_tp(i, carry):
        pl.semaphore_signal(barrier, inc=1, device_id=(g, f, lax.rem(t + i, 8)), device_id_type=MESH)
        return carry

    lax.fori_loop(1, 8, greet_tp, 0)

    loads = [
        pltpu.make_async_copy(routes_hbm, routes_ref, load_sem.at[0]),
        pltpu.make_async_copy(prompt_hbm, prompt_v, load_sem.at[1]),
        pltpu.make_async_copy(gate_hbm, gate_v, load_sem.at[2]),
        pltpu.make_async_copy(up_hbm, up_v, load_sem.at[3]),
        pltpu.make_async_copy(down_hbm, down_v, load_sem.at[4]),
        pltpu.make_async_copy(gain_hbm, gain_ref, load_sem.at[5]),
        pltpu.make_async_copy(rw_hbm, rw_ref, load_sem.at[6]),
    ]
    for ld in loads:
        ld.start()

    def round_d(p):
        def body(i, carry):
            stage_d[p, i] = down_v[i, p].astype(BF)
            return carry

        lax.fori_loop(0, 16, body, 0)
        w_d[p, me] = stage_d[p, f]

    def round_gu(p, gain):
        def body(i, carry):
            stage_gu[p, i, :, 0:128] = (gain * gate_v[i, p]).astype(BF)
            stage_gu[p, i, :, 128:256] = (gain * up_v[i, p]).astype(BF)
            return carry

        lax.fori_loop(0, 16, body, 0)
        w_gu[p][me] = stage_gu[p, f]

    def send_w(stage, dest, sem, rows):
        def body(i, carry):
            gg, ff = at_zy(z + i // 4, y + lax.rem(i, 4))
            pltpu.make_async_remote_copy(
                src_ref=stage.at[ff, rows],
                dst_ref=dest.at[me, rows],
                send_sem=wsend.at[sem],
                recv_sem=wrecv.at[sem],
                device_id=(gg, ff, t),
                device_id_type=MESH,
            ).start()
            return carry

        lax.fori_loop(1, 32, body, 0)

    def await_w(sems, dest, sem, rows):
        part = dest.at[pl.ds(0, 31), rows]
        pltpu.make_async_copy(part, part, sems.at[sem]).wait()

    def copy_to(ref, sems, i, where):
        return pltpu.make_async_remote_copy(
            src_ref=ref,
            dst_ref=ref,
            send_sem=asend.at[sems, i],
            recv_sem=arecv.at[sems, i],
            device_id=where,
            device_id_type=MESH,
        )

    def piece(kind, tt, half):
        p = kind % 2
        if kind < 2:
            ref = tok.at[p, tt]
            return ref if half is None else ref.at[pl.ds(8 * half, 8)]
        ref = hid.at[p, tt]
        return ref if half is None else ref.at[pl.ds(512 * half, 512)]

    def ag_own(kind):
        ref = piece(kind, t, None)
        copy_to(ref, kind, OWN_R, right).start()
        copy_to(ref, kind, OWN_L, left).start()
        copy_to(ref, kind, OWN_C, other).start()

    def ag_relay(kind):
        copy_to(piece(kind, t_l, None), kind, OWN_R, right).wait_recv()
        copy_to(piece(kind, t_l, 0), kind, FAR_R, right).start()
        copy_to(piece(kind, t_l, None), kind, C_L, other).start()
        copy_to(piece(kind, t_r, None), kind, OWN_L, left).wait_recv()
        copy_to(piece(kind, t_r, 1), kind, FAR_L, left).start()
        copy_to(piece(kind, t_r, None), kind, C_R, other).start()

    def ag_far(kind):
        copy_to(piece(kind, t_f, 0), kind, FAR_R, right).wait_recv()
        copy_to(piece(kind, t_f, 0), kind, C_F0, other).start()
        copy_to(piece(kind, t_f, 1), kind, FAR_L, left).wait_recv()
        copy_to(piece(kind, t_f, 1), kind, C_F1, other).start()

    def ag_end(kind):
        for i, half in ((OWN_C, None), (C_L, None), (C_R, None), (C_F0, 0), (C_F1, 1)):
            copy_to(piece(kind, t, half), kind, i, other).wait_recv()

    def ag_drain(kind):
        for i, half in (
            (OWN_R, None),
            (OWN_L, None),
            (OWN_C, None),
            (FAR_R, 0),
            (FAR_L, 1),
            (C_L, None),
            (C_R, None),
            (C_F0, 0),
            (C_F1, 1),
        ):
            copy_to(piece(kind, t, half), kind, i, other).wait_send()

    def send_tokens(p):
        for j, dz, lo, hi in PLANES:
            for dy in range(4):
                gg, ff = at_zy(z + dz, y + dy)
                if dz == 0 and dy == 0:
                    continue
                pltpu.make_async_remote_copy(
                    src_ref=slots_x.at[p, ff, pl.ds(lo, hi - lo)],
                    dst_ref=tok.at[p, t, j * 4 + y, pl.ds(lo, hi - lo)],
                    send_sem=tsend.at[p],
                    recv_sem=trecv.at[p],
                    device_id=(gg, ff, t),
                    device_id_type=MESH,
                ).start()
        tok[p, t, y] = slots_x[p, f]

    def await_tokens(sems, p):
        part = slots_x.at[p, pl.ds(0, 15)]
        pltpu.make_async_copy(part, part, sems.at[p]).wait()

    def send_back(p, plane, sem, lanes):
        for j, dz, lo, hi in PLANES:
            for dy in range(4):
                if j != plane or (dz == 0 and dy == 0):
                    continue
                gg, ff = at_zy(z - dz, y + dy)
                pltpu.make_async_remote_copy(
                    src_ref=outs.at[p, j * 4 + lax.rem(y + dy, 4), pl.ds(lo, hi - lo), lanes],
                    dst_ref=ans.at[p, f, pl.ds(lo, hi - lo), lanes],
                    send_sem=rsend.at[sem],
                    recv_sem=rrecv.at[sem],
                    device_id=(gg, ff, t),
                    device_id_type=MESH,
                ).start()
        if plane == 0:
            ans[p, f, :, lanes] = outs[p, y, :, lanes]

    def await_back(sems, p, sem, lanes):
        part = outs.at[p, pl.ds(0, 15), :, lanes]
        pltpu.make_async_copy(part, part, sems.at[sem]).wait()

    def send_dx(p, h):
        def body(i, carry):
            tt = lax.rem(t + i, 8)
            pltpu.make_async_remote_copy(
                src_ref=w_d.at[p, pl.ds(tt * 4, 4), pl.ds(32 * h, 32)],
                dst_ref=dx.at[p, h, t],
                send_sem=dsend.at[p, h],
                recv_sem=drecv.at[p, h],
                device_id=(g, f, tt),
                device_id_type=MESH,
            ).start()
            return carry

        lax.fori_loop(1, 8, body, 0)
        dx[p, h, t] = w_d[p, pl.ds(t * 4, 4), pl.ds(32 * h, 32)]

    def await_dx(sems, p, h):
        part = dx.at[p, h, pl.ds(0, 7)]
        pltpu.make_async_copy(part, part, sems.at[p, h]).wait()

    def hidden(p):
        def body(r, carry):
            rows = jnp.concatenate(
                [tok[p, tt, pl.ds(r * 4, 4)].reshape(256, 256) for tt in range(8)], axis=1
            )
            pre = jnp.dot(rows, w_gu[p][...].reshape(2048, 256), preferred_element_type=F32) * 2048 ** (-0.5)
            gate, up = pre[:, 0:128], pre[:, 128:256]
            value = gate / (1.0 + jnp.exp(-gate)) * up
            hid[p, t, pl.ds(r * 256, 256)] = value.astype(BF)
            return carry

        lax.fori_loop(0, 4, body, 0)

    def expert_out(p, halves, sem, lanes):
        for r in (3, 1, 2, 0):
            rows = jnp.concatenate([hid[p, tt, pl.ds(r * 256, 256)] for tt in range(8)], axis=1)
            cols = jnp.concatenate(
                [
                    jnp.concatenate([dx[p, h, tt].reshape(128, 128) for tt in range(8)], axis=1)
                    for h in halves
                ],
                axis=0,
            )
            value = lax.dot_general(rows, cols, (((1,), (1,)), ((), ())), preferred_element_type=F32)
            value = (value * 1024 ** (-0.5)).astype(BF)
            outs[p, pl.ds(r * 4, 4), :, lanes] = value.reshape(4, 64, 128 * len(halves))
            send_back(p, r, sem, lanes)

    def blend(p, lanes):
        for r in range(2):
            rows = pl.ds(r * 256, 256)
            here = slice(r * 256, r * 256 + 256)
            values = ans[p, :, :, lanes].reshape(1024, lanes.size)
            first = jnp.dot(s0[p, rows], values, preferred_element_type=F32)
            second = jnp.dot(s1[p, rows], values, preferred_element_type=F32)
            part = rw0[here] * first + rw1[here] * second
            if p == 0:
                acc[rows] = part
            else:
                acc[rows, lanes] += part

    def place_columns():
        a = lax.broadcasted_iota(jnp.int32, (256, 256), 0)
        b = lax.broadcasted_iota(jnp.int32, (256, 256), 1)
        goes = a == ((b >> 5) & 1) * 128 + (b >> 6) * 32 + (b & 31)
        to_place = jnp.where(goes, 1.0, 0.0).astype(BF)
        blend_v[...] = jnp.dot(acc[...].astype(BF), to_place, preferred_element_type=F32).astype(BF)

    whole = pl.ds(0, 256)
    low, high = pl.ds(0, 128), pl.ds(128, 128)
    all_rows = pl.ds(0, 64)
    rows_a, rows_b = pl.ds(0, 32), pl.ds(32, 32)

    loads[0].wait()
    row_i = lax.broadcasted_iota(jnp.int32, (512, 512), 0)
    col_i = lax.broadcasted_iota(jnp.int32, (512, 512), 1)
    diag = col_i == row_i

    def column(row):
        return jnp.sum(jnp.where(diag, row, 0.0), axis=1, keepdims=True)

    experts = lax.broadcasted_iota(jnp.int32, (32, 512), 0)
    hit0 = jnp.where(routes_ref[0:1] == experts, 1.0, 0.0)
    hit1 = jnp.where(routes_ref[1:2] == experts, 1.0, 0.0)
    before = jnp.where(row_i < col_i, 1.0, 0.0).astype(BF)
    rank0 = jnp.dot(hit0.astype(BF), before, preferred_element_type=F32)
    rank1 = jnp.dot(hit1.astype(BF), before, preferred_element_type=F32) + jnp.sum(hit0, axis=1, keepdims=True)
    place = ((experts >> 1) * 64 + (experts & 1) * 1024).astype(F32)
    slot0_row = jnp.sum((rank0 + place) * hit0, axis=0, keepdims=True)
    slot1_row = jnp.sum((rank1 + place) * hit1, axis=0, keepdims=True)

    loads[1].wait()
    wide = prompt_v[...].astype(F32)
    scale = lax.rsqrt(jnp.sum(wide * wide, axis=1, keepdims=True) * (1.0 / 2048) + EPS)
    mine = prompt_v[:, pl.ds(pl.multiple_of(t * 256, 256), 256)].astype(F32)
    normed = (mine * scale).astype(BF)

    def pick_slots(p):
        for r in range(4):
            number = (lax.broadcasted_iota(jnp.int32, (256, 512), 0) + (p * 1024 + r * 256)).astype(F32)
            pick = jnp.where((number == slot0_row) | (number == slot1_row), 1.0, 0.0).astype(BF)
            rows = jnp.dot(pick, normed, preferred_element_type=F32).astype(BF)
            slots_x[p, pl.ds(r * 4, 4)] = rows.reshape(4, 64, 256)

    pick_slots(0)
    pick_slots(1)
    loads[4].wait()
    round_d(0)
    pl.semaphore_wait(barrier, 38)
    send_tokens(0)
    send_tokens(1)
    send_w(stage_d.at[0], w_d.at[0], 0, all_rows)
    loads[2].wait()
    loads[3].wait()
    loads[5].wait()
    eye = lax.broadcasted_iota(jnp.int32, (64, 64), 0) == lax.broadcasted_iota(jnp.int32, (64, 64), 1)
    gain = jnp.sum(jnp.where(eye, gain_ref[...], 0.0), axis=1, keepdims=True)
    round_gu(0, gain)
    send_w(stage_gu.at[0], w_gu0, 2, all_rows)
    round_gu(1, gain)
    send_w(stage_gu.at[1], w_gu1, 3, all_rows)
    round_d(1)
    send_w(stage_d.at[1], w_d.at[1], 1, rows_a)
    await_tokens(trecv, 0)
    ag_own(TOK0)
    await_tokens(trecv, 1)
    ag_own(TOK1)
    slot0 = column(slot0_row)
    slot1 = column(slot1_row)
    for p in range(2):
        number = (lax.broadcasted_iota(jnp.int32, (512, 1024), 1) + p * 1024).astype(F32)
        s0[p] = jnp.where(number == slot0, 1.0, 0.0).astype(BF)
        s1[p] = jnp.where(number == slot1, 1.0, 0.0).astype(BF)
    loads[6].wait()
    rw0 = column(rw_ref[0:1])
    rw1 = column(rw_ref[1:2])
    ag_relay(TOK0)
    ag_relay(TOK1)
    ag_far(TOK0)
    ag_far(TOK1)
    ag_end(TOK0)
    ag_end(TOK1)
    await_w(wrecv, w_d.at[0], 0, all_rows)
    send_dx(0, 0)
    send_dx(0, 1)
    await_w(wrecv, w_gu0, 2, all_rows)
    hidden(0)
    ag_own(HID0)
    ag_relay(HID0)
    ag_far(HID0)
    await_dx(drecv, 0, 0)
    await_dx(drecv, 0, 1)
    ag_end(HID0)
    expert_out(0, (0, 1), 0, whole)
    send_w(stage_d.at[1], w_d.at[1], 4, rows_b)
    await_w(wrecv, w_gu1, 3, all_rows)
    hidden(1)
    ag_own(HID1)
    ag_relay(HID1)
    ag_far(HID1)
    await_w(wrecv, w_d.at[1], 1, rows_a)
    send_dx(1, 0)
    ag_end(HID1)
    await_back(rrecv, 0, 0, whole)
    blend(0, whole)
    await_w(wrecv, w_d.at[1], 4, rows_b)
    send_dx(1, 1)
    await_dx(drecv, 1, 0)
    expert_out(1, (0,), 1, low)
    await_dx(drecv, 1, 1)
    expert_out(1, (1,), 2, high)
    for kind in range(4):
        ag_drain(kind)
    for p in range(2):
        await_tokens(tsend, p)
        for h in range(2):
            await_dx(dsend, p, h)
    await_w(wsend, w_d.at[0], 0, all_rows)
    await_w(wsend, w_d.at[1], 1, rows_a)
    await_w(wsend, w_gu0, 2, all_rows)
    await_w(wsend, w_gu1, 3, all_rows)
    await_w(wsend, w_d.at[1], 4, rows_b)
    await_back(rsend, 0, 0, whole)
    await_back(rrecv, 1, 1, low)
    blend(1, low)
    await_back(rrecv, 1, 2, high)
    blend(1, high)
    place_columns()
    await_back(rsend, 1, 1, low)
    await_back(rsend, 1, 2, high)


def copy_out(w_gu0, w_gu1, w_d, blend_v, gate_out, up_out, down_out, blend_out, sem):
    copies = [
        pltpu.make_async_copy(w_gu0.at[:, :, pl.ds(0, 128)], gate_out.at[0], sem.at[0]),
        pltpu.make_async_copy(w_gu1.at[:, :, pl.ds(0, 128)], gate_out.at[1], sem.at[1]),
        pltpu.make_async_copy(w_gu0.at[:, :, pl.ds(128, 128)], up_out.at[0], sem.at[2]),
        pltpu.make_async_copy(w_gu1.at[:, :, pl.ds(128, 128)], up_out.at[1], sem.at[3]),
        pltpu.make_async_copy(w_d, down_out, sem.at[4]),
        pltpu.make_async_copy(blend_v, blend_out, sem.at[5]),
    ]
    for cp in copies:
        cp.start()
    for cp in copies:
        cp.wait()


def per_device(prompt, norm_gain, gate_master, up_master, down_master, routes, route_weights):
    hbm = pl.BlockSpec(memory_space=pltpu.HBM)
    vmem = pl.BlockSpec(memory_space=pltpu.VMEM)
    ready = jax.ShapeDtypeStruct((2, 32, 64, 128), BF)
    both = jax.ShapeDtypeStruct((32, 64, 256), BF)
    block = jax.ShapeDtypeStruct((512, 256), BF)
    dma = pltpu.SemaphoreType.DMA
    split = lambda a: a.reshape(16, 2, 64, 128)
    w_gu0, w_gu1, w_d, out = pl.pallas_call(
        kernel,
        out_shape=(both, both, ready, block),
        in_specs=[hbm] * 7,
        out_specs=(vmem,) * 4,
        scratch_shapes=[
            pltpu.VMEM((1, 64), F32),
            pltpu.VMEM((2, 512), jnp.int32),
            pltpu.VMEM((2, 512), F32),
            pltpu.VMEM((512, 2048), BF),
            pltpu.VMEM((16, 2, 64, 128), F32),
            pltpu.VMEM((16, 2, 64, 128), F32),
            pltpu.VMEM((16, 2, 64, 128), F32),
            pltpu.VMEM((2, 16, 64, 256), BF),
            pltpu.VMEM((2, 16, 64, 128), BF),
            pltpu.VMEM((2, 16, 64, 256), BF),
            pltpu.VMEM((2, 8, 16, 64, 256), BF),
            pltpu.VMEM((2, 8, 1024, 128), BF),
            pltpu.VMEM((2, 2, 8, 4, 32, 128), BF),
            pltpu.VMEM((2, 16, 64, 256), BF),
            pltpu.VMEM((2, 16, 64, 256), BF),
            pltpu.VMEM((2, 512, 1024), BF),
            pltpu.VMEM((2, 512, 1024), BF),
            pltpu.VMEM((512, 256), F32),
            dma((7,)),
            dma((5,)),
            dma((5,)),
            dma((2,)),
            dma((2,)),
            dma((4, 9)),
            dma((4, 9)),
            dma((2, 2)),
            dma((2, 2)),
            dma((3,)),
            dma((3,)),
        ],
        compiler_params=pltpu.CompilerParams(
            collective_id=0, has_side_effects=True, vmem_limit_bytes=50 * 2**20
        ),
    )(
        prompt,
        norm_gain.reshape(1, 64),
        split(gate_master),
        split(up_master),
        split(down_master),
        routes.T,
        route_weights.T,
    )
    gate, up, down, out = pl.pallas_call(
        copy_out,
        out_shape=(ready, ready, ready, block),
        in_specs=[vmem] * 4,
        out_specs=(hbm,) * 4,
        scratch_shapes=[dma((6,))],
        compiler_params=pltpu.CompilerParams(vmem_limit_bytes=16 * 2**20),
    )(w_gu0, w_gu1, w_d, out)
    flat = lambda a: a.reshape(2, 2048, 128)
    return flat(gate), flat(up), flat(down), out


def solution(mesh):
    in_specs = (
        P(("gr", "fs"), None),
        P(("gr", "fs")),
        P(None, ("gr", "fs"), "tp"),
        P(None, ("gr", "fs"), "tp"),
        P(None, ("gr", "fs"), "tp"),
        P(("gr", "fs"), None),
        P(("gr", "fs"), None),
    )
    out_specs = (
        P("fs", None, "tp"),
        P("fs", None, "tp"),
        P("fs", None, "tp"),
        P(("gr", "fs"), "tp"),
    )
    return jax.shard_map(
        per_device, mesh=mesh, in_specs=in_specs, out_specs=out_specs, check_vma=False
    )
```

```python
import jax
import jax.numpy as jnp
from jax import lax
from jax.experimental import pallas as pl
from jax.experimental.pallas import tpu as pltpu
from jax.sharding import PartitionSpec as P

MESH = pl.DeviceIdType.MESH
EPS = 1e-06
BF = jnp.bfloat16
F32 = jnp.float32

PLANES = ((0, 0, 0, 64), (1, 1, 0, 64), (2, -1, 0, 64), (3, 2, 0, 32), (3, -2, 32, 64))
TOK0, TOK1, HID0, HID1 = 0, 1, 2, 3
OWN_R0, OWN_R1, OWN_L0, OWN_L1, OWN_C, FAR_R, FAR_L, C_L, C_R, C_F0, C_F1 = range(11)


def kernel(
    prompt_hbm,
    gain_hbm,
    gate_hbm,
    up_hbm,
    down_hbm,
    routes_hbm,
    rw_hbm,
    w_gu0,
    w_gu1,
    w_d,
    hi1,
    lo1,
    acc,
    ansb,
    gain_ref,
    routes_ref,
    rw_ref,
    prompt_v,
    gate_v,
    up_v,
    down_v,
    stage_gu,
    stage_d,
    slots_x,
    tok,
    hid,
    dx,
    outs,
    ans,
    ansa,
    hi0,
    lo0,
    load_sem,
    wsend,
    wrecv,
    tsend,
    trecv,
    asend,
    arecv,
    dsend,
    drecv,
    rsend,
    rrecv,
):
    w_gu = (w_gu0, w_gu1)
    g = lax.axis_index("gr")
    f = lax.axis_index("fs")
    t = lax.axis_index("tp")
    me = g * 16 + f
    z = g * 4 + (f >> 2)
    y = f & 3
    x = t >> 1
    c = t & 1

    def at_zy(zz, yy):
        zz = (zz + 8) & 7
        yy = (yy + 4) & 3
        return zz >> 2, ((zz & 3) << 2) + yy

    right = (g, f, ((x + 1) & 3) * 2 + c)
    left = (g, f, ((x + 3) & 3) * 2 + c)
    other = (g, f, x * 2 + 1 - c)
    t_l = ((x + 3) & 3) * 2 + c
    t_r = ((x + 1) & 3) * 2 + c
    t_f = ((x + 2) & 3) * 2 + c

    barrier = pltpu.get_barrier_semaphore()

    def greet_zy(i, carry):
        gg, ff = at_zy(z + (i >> 2), y + (i & 3))
        pl.semaphore_signal(barrier, inc=1, device_id=(gg, ff, t), device_id_type=MESH)
        return carry

    lax.fori_loop(1, 32, greet_zy, 0)

    def greet_tp(i, carry):
        pl.semaphore_signal(barrier, inc=1, device_id=(g, f, (t + i) & 7), device_id_type=MESH)
        return carry

    lax.fori_loop(1, 8, greet_tp, 0)

    loads = [
        pltpu.make_async_copy(routes_hbm, routes_ref, load_sem.at[0]),
        pltpu.make_async_copy(prompt_hbm, prompt_v, load_sem.at[1]),
        pltpu.make_async_copy(gate_hbm, gate_v, load_sem.at[2]),
        pltpu.make_async_copy(up_hbm, up_v, load_sem.at[3]),
        pltpu.make_async_copy(down_hbm, down_v, load_sem.at[4]),
        pltpu.make_async_copy(gain_hbm, gain_ref, load_sem.at[5]),
        pltpu.make_async_copy(rw_hbm, rw_ref, load_sem.at[6]),
    ]
    for ld in loads:
        ld.start()

    def round_d(p):
        def body(i, carry):
            stage_d[p, i] = down_v[i, p].astype(BF)
            return carry

        lax.fori_loop(0, 16, body, 0)
        w_d[p, me] = stage_d[p, f]

    def round_gu(p, gain):
        def body(i, carry):
            stage_gu[p, i, :, 0:128] = (gain * gate_v[i, p]).astype(BF)
            stage_gu[p, i, :, 128:256] = (gain * up_v[i, p]).astype(BF)
            return carry

        lax.fori_loop(0, 16, body, 0)
        w_gu[p][me] = stage_gu[p, f]

    def send_w(stage, dest, sem, rows):
        def body(i, carry):
            gg, ff = at_zy(z + (i >> 2), y + (i & 3))
            pltpu.make_async_remote_copy(
                src_ref=stage.at[ff, rows],
                dst_ref=dest.at[me, rows],
                send_sem=wsend.at[sem],
                recv_sem=wrecv.at[sem],
                device_id=(gg, ff, t),
                device_id_type=MESH,
            ).start()
            return carry

        lax.fori_loop(1, 32, body, 0)

    def await_w(sems, dest, sem, rows):
        part = dest.at[pl.ds(0, 31), rows]
        pltpu.make_async_copy(part, part, sems.at[sem]).wait()

    def copy_to(ref, sems, i, where):
        return pltpu.make_async_remote_copy(
            src_ref=ref,
            dst_ref=ref,
            send_sem=asend.at[sems, i],
            recv_sem=arecv.at[sems, i],
            device_id=where,
            device_id_type=MESH,
        )

    def piece(kind, tt, half):
        p = kind % 2
        if kind < 2:
            ref = tok.at[p, tt]
            return ref if half is None else ref.at[pl.ds(8 * half, 8)]
        ref = hid.at[p, tt]
        return ref if half is None else ref.at[pl.ds(512 * half, 512)]

    def ag_own(kind):
        copy_to(piece(kind, t, 0), kind, OWN_R0, right).start()
        copy_to(piece(kind, t, 1), kind, OWN_L1, left).start()
        copy_to(piece(kind, t, 1), kind, OWN_R1, right).start()
        copy_to(piece(kind, t, 0), kind, OWN_L0, left).start()
        copy_to(piece(kind, t, None), kind, OWN_C, other).start()

    def ag_relay(kind):
        copy_to(piece(kind, t_l, 0), kind, OWN_R0, right).wait_recv()
        copy_to(piece(kind, t_l, 0), kind, FAR_R, right).start()
        copy_to(piece(kind, t_r, 1), kind, OWN_L1, left).wait_recv()
        copy_to(piece(kind, t_r, 1), kind, FAR_L, left).start()

    def ag_pass(kind):
        copy_to(piece(kind, t_l, 1), kind, OWN_R1, right).wait_recv()
        copy_to(piece(kind, t_l, None), kind, C_L, other).start()
        copy_to(piece(kind, t_r, 0), kind, OWN_L0, left).wait_recv()
        copy_to(piece(kind, t_r, None), kind, C_R, other).start()

    def ag_far(kind):
        copy_to(piece(kind, t_f, 0), kind, FAR_R, right).wait_recv()
        copy_to(piece(kind, t_f, 0), kind, C_F0, other).start()
        copy_to(piece(kind, t_f, 1), kind, FAR_L, left).wait_recv()
        copy_to(piece(kind, t_f, 1), kind, C_F1, other).start()

    def ag_end(kind):
        for i, half in ((OWN_C, None), (C_L, None), (C_R, None), (C_F0, 0), (C_F1, 1)):
            copy_to(piece(kind, t, half), kind, i, other).wait_recv()

    def ag_drain(kind):
        for i in (OWN_C, C_L, C_R):
            copy_to(piece(kind, t, None), kind, i, other).wait_send()
        for i in (OWN_R0, OWN_R1, OWN_L0, OWN_L1, FAR_R, FAR_L, C_F0, C_F1):
            copy_to(piece(kind, t, 0), kind, i, other).wait_send()

    def send_tokens(p):
        for j, dz, lo, hi in PLANES:
            for dy in range(4):
                gg, ff = at_zy(z + dz, y + dy)
                if dz == 0 and dy == 0:
                    continue
                pltpu.make_async_remote_copy(
                    src_ref=slots_x.at[p, ff, pl.ds(lo, hi - lo)],
                    dst_ref=tok.at[p, t, j * 4 + y, pl.ds(lo, hi - lo)],
                    send_sem=tsend.at[p],
                    recv_sem=trecv.at[p],
                    device_id=(gg, ff, t),
                    device_id_type=MESH,
                ).start()
        tok[p, t, y] = slots_x[p, f]

    def await_tokens(sems, p):
        part = slots_x.at[p, pl.ds(0, 15)]
        pltpu.make_async_copy(part, part, sems.at[p]).wait()

    def back(p, sem):
        return (ans, ansa, ansb)[sem]

    def send_back(p, plane, sem, lanes):
        for j, dz, lo, hi in PLANES:
            for dy in range(4):
                if j != plane or (dz == 0 and dy == 0):
                    continue
                gg, ff = at_zy(z - dz, y + dy)
                pltpu.make_async_remote_copy(
                    src_ref=outs.at[p, j * 4 + ((y + dy) & 3), pl.ds(lo, hi - lo), lanes],
                    dst_ref=back(p, sem).at[f, pl.ds(lo, hi - lo)],
                    send_sem=rsend.at[sem],
                    recv_sem=rrecv.at[sem],
                    device_id=(gg, ff, t),
                    device_id_type=MESH,
                ).start()
        if plane == 0:
            back(p, sem)[f] = outs[p, y, :, lanes]

    def await_back(sems, p, sem, lanes):
        part = outs.at[p, pl.ds(0, 15), :, lanes]
        pltpu.make_async_copy(part, part, sems.at[sem]).wait()

    def send_dx(p, h):
        def body(i, carry):
            tt = (t + i) & 7
            pltpu.make_async_remote_copy(
                src_ref=w_d.at[p, pl.ds(tt * 4, 4), pl.ds(32 * h, 32)],
                dst_ref=dx.at[p, h, t],
                send_sem=dsend.at[p, h],
                recv_sem=drecv.at[p, h],
                device_id=(g, f, tt),
                device_id_type=MESH,
            ).start()
            return carry

        lax.fori_loop(1, 8, body, 0)
        dx[p, h, t] = w_d[p, pl.ds(t * 4, 4), pl.ds(32 * h, 32)]

    def await_dx(sems, p, h):
        part = dx.at[p, h, pl.ds(0, 7)]
        pltpu.make_async_copy(part, part, sems.at[p, h]).wait()

    def hidden(p):
        def body(r, carry):
            rows = jnp.concatenate(
                [tok[p, tt, pl.ds(r * 4, 4)].reshape(256, 256) for tt in range(8)], axis=1
            )
            pre = jnp.dot(rows, w_gu[p][...].reshape(2048, 256), preferred_element_type=F32) * 2048 ** (-0.5)
            gate, up = pre[:, 0:128], pre[:, 128:256]
            value = gate / (1.0 + jnp.exp(-gate)) * up
            hid[p, t, pl.ds(r * 256, 256)] = value.astype(BF)
            return carry

        lax.fori_loop(0, 4, body, 0)

    def expert_out(p, halves, sem, lanes):
        for r in (3, 1, 2, 0):
            rows = jnp.concatenate([hid[p, tt, pl.ds(r * 256, 256)] for tt in range(8)], axis=1)
            cols = jnp.concatenate(
                [
                    jnp.concatenate([dx[p, h, tt].reshape(128, 128) for tt in range(8)], axis=1)
                    for h in halves
                ],
                axis=0,
            )
            value = lax.dot_general(rows, cols, (((1,), (1,)), ((), ())), preferred_element_type=F32)
            value = (value * 1024 ** (-0.5)).astype(BF)
            outs[p, pl.ds(r * 4, 4), :, lanes] = value.reshape(4, 64, 128 * len(halves))
            send_back(p, r, sem, lanes)

    def blend(p, sem, lanes):
        for r in range(2):
            rows = pl.ds(r * 256, 256)
            values = back(p, sem)[...].reshape(1024, lanes.size)
            part = jnp.dot((hi0, hi1)[p][rows], values, preferred_element_type=F32)
            part += jnp.dot((lo0, lo1)[p][rows], values, preferred_element_type=F32)
            if p == 0:
                acc[rows] = part
            else:
                acc[rows, lanes] += part

    whole = pl.ds(0, 256)
    low, high = pl.ds(0, 128), pl.ds(128, 128)
    all_rows = pl.ds(0, 64)
    rows_a, rows_b = pl.ds(0, 32), pl.ds(32, 32)

    loads[0].wait()
    row_i = lax.broadcasted_iota(jnp.int32, (512, 512), 0)
    col_i = lax.broadcasted_iota(jnp.int32, (512, 512), 1)
    diag = col_i == row_i

    def column(row):
        return jnp.sum(jnp.where(diag, row, 0.0), axis=1, keepdims=True)

    experts = lax.broadcasted_iota(jnp.int32, (32, 512), 0)
    hit0 = jnp.where(routes_ref[0:1] == experts, 1.0, 0.0)
    hit1 = jnp.where(routes_ref[1:2] == experts, 1.0, 0.0)
    before = jnp.where(row_i < col_i, 1.0, 0.0).astype(BF)
    rank0 = jnp.dot(hit0.astype(BF), before, preferred_element_type=F32)
    rank1 = jnp.dot(hit1.astype(BF), before, preferred_element_type=F32) + jnp.sum(hit0, axis=1, keepdims=True)
    place = ((experts >> 1) * 64 + (experts & 1) * 1024).astype(F32)
    slot0_row = jnp.sum((rank0 + place) * hit0, axis=0, keepdims=True)
    slot1_row = jnp.sum((rank1 + place) * hit1, axis=0, keepdims=True)

    loads[1].wait()
    wide = prompt_v[...].astype(F32)
    scale = lax.rsqrt(jnp.sum(wide * wide, axis=1, keepdims=True) * (1.0 / 2048) + EPS)
    mine = prompt_v[:, pl.ds(pl.multiple_of(t * 256, 256), 256)].astype(F32)
    normed = (mine * scale).astype(BF)

    def pick_slots(p):
        for r in range(4):
            number = (lax.broadcasted_iota(jnp.int32, (256, 512), 0) + (p * 1024 + r * 256)).astype(F32)
            pick = jnp.where((number == slot0_row) | (number == slot1_row), 1.0, 0.0).astype(BF)
            rows = jnp.dot(pick, normed, preferred_element_type=F32).astype(BF)
            slots_x[p, pl.ds(r * 4, 4)] = rows.reshape(4, 64, 256)

    pick_slots(0)
    pick_slots(1)
    loads[4].wait()
    round_d(0)
    pl.semaphore_wait(barrier, 38)
    send_tokens(0)
    send_tokens(1)
    loads[2].wait()
    loads[3].wait()
    loads[5].wait()
    eye = lax.broadcasted_iota(jnp.int32, (64, 64), 0) == lax.broadcasted_iota(jnp.int32, (64, 64), 1)
    gain = jnp.sum(jnp.where(eye, gain_ref[...], 0.0), axis=1, keepdims=True)
    round_gu(0, gain)
    send_w(stage_gu.at[0], w_gu0, 2, all_rows)
    round_gu(1, gain)
    send_w(stage_gu.at[1], w_gu1, 3, all_rows)
    send_w(stage_d.at[0], w_d.at[0], 0, all_rows)
    round_d(1)
    send_w(stage_d.at[1], w_d.at[1], 1, rows_a)
    send_w(stage_d.at[1], w_d.at[1], 4, rows_b)
    await_tokens(trecv, 0)
    ag_own(TOK0)
    await_tokens(trecv, 1)
    ag_own(TOK1)
    loads[6].wait()
    slot0 = column(slot0_row)
    slot1 = column(slot1_row)
    rw0 = column(rw_ref[0:1])
    rw1 = column(rw_ref[1:2])
    for p in range(2):
        for r in range(4):
            cols = pl.ds(r * 256, 256)
            number = (lax.broadcasted_iota(jnp.int32, (512, 256), 1) + (p * 1024 + r * 256)).astype(F32)
            weight = jnp.where(number == slot0, rw0, jnp.where(number == slot1, rw1, 0.0))
            upper = weight.astype(BF)
            (hi0, hi1)[p][:, cols] = upper
            (lo0, lo1)[p][:, cols] = (weight - upper.astype(F32)).astype(BF)
    ag_relay(TOK0)
    ag_pass(TOK0)
    ag_relay(TOK1)
    ag_far(TOK0)
    ag_pass(TOK1)
    ag_far(TOK1)
    ag_end(TOK0)
    await_w(wrecv, w_gu0, 2, all_rows)
    hidden(0)
    ag_own(HID0)
    ag_end(TOK1)
    ag_relay(HID0)
    ag_pass(HID0)
    ag_far(HID0)
    ag_end(HID0)
    await_w(wrecv, w_gu1, 3, all_rows)
    hidden(1)
    ag_own(HID1)
    ag_relay(HID1)
    ag_pass(HID1)
    await_w(wrecv, w_d.at[0], 0, all_rows)
    send_dx(0, 0)
    send_dx(0, 1)
    ag_far(HID1)
    ag_end(HID1)
    await_dx(drecv, 0, 0)
    await_dx(drecv, 0, 1)
    expert_out(0, (0, 1), 0, whole)
    await_w(wrecv, w_d.at[1], 1, rows_a)
    send_dx(1, 0)
    await_w(wrecv, w_d.at[1], 4, rows_b)
    send_dx(1, 1)
    await_dx(drecv, 1, 0)
    expert_out(1, (0,), 1, low)
    await_dx(drecv, 1, 1)
    expert_out(1, (1,), 2, high)
    for kind in range(4):
        ag_drain(kind)
    for p in range(2):
        await_tokens(tsend, p)
        for h in range(2):
            await_dx(dsend, p, h)
    await_w(wsend, w_d.at[0], 0, all_rows)
    await_w(wsend, w_d.at[1], 1, rows_a)
    await_w(wsend, w_gu0, 2, all_rows)
    await_w(wsend, w_gu1, 3, all_rows)
    await_w(wsend, w_d.at[1], 4, rows_b)
    await_back(rrecv, 0, 0, whole)
    blend(0, 0, whole)
    await_back(rsend, 0, 0, whole)
    await_back(rrecv, 1, 1, low)
    blend(1, 1, low)
    await_back(rsend, 1, 1, low)
    await_back(rsend, 1, 2, high)
    await_back(rrecv, 1, 2, high)


def copy_out(
    w_gu0,
    w_gu1,
    w_d,
    hi1,
    lo1,
    acc,
    ansb,
    gate_out,
    up_out,
    down_out,
    blend_out,
    blend_v,
    sem,
):
    copies = [
        pltpu.make_async_copy(w_gu0.at[:, :, pl.ds(0, 128)], gate_out.at[0], sem.at[0]),
        pltpu.make_async_copy(w_gu1.at[:, :, pl.ds(0, 128)], gate_out.at[1], sem.at[1]),
        pltpu.make_async_copy(w_gu0.at[:, :, pl.ds(128, 128)], up_out.at[0], sem.at[2]),
        pltpu.make_async_copy(w_gu1.at[:, :, pl.ds(128, 128)], up_out.at[1], sem.at[3]),
        pltpu.make_async_copy(w_d, down_out, sem.at[4]),
        pltpu.make_async_copy(blend_v, blend_out, sem.at[5]),
    ]
    for cp in copies[:5]:
        cp.start()
    a = lax.broadcasted_iota(jnp.int32, (256, 256), 0)
    b = lax.broadcasted_iota(jnp.int32, (256, 256), 1)
    goes = a == ((b >> 5) & 1) * 128 + (b >> 6) * 32 + (b & 31)
    to_place = jnp.where(goes, 1.0, 0.0).astype(BF)
    values = ansb[...].reshape(1024, 128)
    part = jnp.dot(hi1[...], values, preferred_element_type=F32)
    part += jnp.dot(lo1[...], values, preferred_element_type=F32)
    total = jnp.concatenate([acc[:, 0:128], acc[:, 128:256] + part], axis=1).astype(BF)
    blend_v[...] = jnp.dot(total, to_place, preferred_element_type=F32).astype(BF)
    copies[5].start()
    for cp in copies:
        cp.wait()


def per_device(prompt, norm_gain, gate_master, up_master, down_master, routes, route_weights):
    hbm = pl.BlockSpec(memory_space=pltpu.HBM)
    vmem = pl.BlockSpec(memory_space=pltpu.VMEM)
    ready = jax.ShapeDtypeStruct((2, 32, 64, 128), BF)
    both = jax.ShapeDtypeStruct((32, 64, 256), BF)
    block = jax.ShapeDtypeStruct((512, 256), BF)
    select = jax.ShapeDtypeStruct((512, 1024), BF)
    total = jax.ShapeDtypeStruct((512, 256), F32)
    part = jax.ShapeDtypeStruct((16, 64, 128), BF)
    dma = pltpu.SemaphoreType.DMA
    split = lambda a: a.reshape(16, 2, 64, 128)
    passed = pl.pallas_call(
        kernel,
        out_shape=(both, both, ready, select, select, total, part),
        in_specs=[hbm] * 7,
        out_specs=(vmem,) * 7,
        scratch_shapes=[
            pltpu.VMEM((1, 64), F32),
            pltpu.VMEM((2, 512), jnp.int32),
            pltpu.VMEM((2, 512), F32),
            pltpu.VMEM((512, 2048), BF),
            pltpu.VMEM((16, 2, 64, 128), F32),
            pltpu.VMEM((16, 2, 64, 128), F32),
            pltpu.VMEM((16, 2, 64, 128), F32),
            pltpu.VMEM((2, 16, 64, 256), BF),
            pltpu.VMEM((2, 16, 64, 128), BF),
            pltpu.VMEM((2, 16, 64, 256), BF),
            pltpu.VMEM((2, 8, 16, 64, 256), BF),
            pltpu.VMEM((2, 8, 1024, 128), BF),
            pltpu.VMEM((2, 2, 8, 4, 32, 128), BF),
            pltpu.VMEM((2, 16, 64, 256), BF),
            pltpu.VMEM((16, 64, 256), BF),
            pltpu.VMEM((16, 64, 128), BF),
            pltpu.VMEM((512, 1024), BF),
            pltpu.VMEM((512, 1024), BF),
            dma((7,)),
            dma((5,)),
            dma((5,)),
            dma((2,)),
            dma((2,)),
            dma((4, 11)),
            dma((4, 11)),
            dma((2, 2)),
            dma((2, 2)),
            dma((3,)),
            dma((3,)),
        ],
        compiler_params=pltpu.CompilerParams(
            collective_id=0, has_side_effects=True, vmem_limit_bytes=48 * 2**20
        ),
    )(
        prompt,
        norm_gain.reshape(1, 64),
        split(gate_master),
        split(up_master),
        split(down_master),
        routes.T,
        route_weights.T,
    )
    gate, up, down, out = pl.pallas_call(
        copy_out,
        out_shape=(ready, ready, ready, block),
        in_specs=[vmem] * 7,
        out_specs=(hbm,) * 4,
        scratch_shapes=[pltpu.VMEM((512, 256), BF), dma((6,))],
        compiler_params=pltpu.CompilerParams(vmem_limit_bytes=16 * 2**20),
    )(*passed)
    flat = lambda a: a.reshape(2, 2048, 128)
    return flat(gate), flat(up), flat(down), out


def solution(mesh):
    in_specs = (
        P(("gr", "fs"), None),
        P(("gr", "fs")),
        P(None, ("gr", "fs"), "tp"),
        P(None, ("gr", "fs"), "tp"),
        P(None, ("gr", "fs"), "tp"),
        P(("gr", "fs"), None),
        P(("gr", "fs"), None),
    )
    out_specs = (
        P("fs", None, "tp"),
        P("fs", None, "tp"),
        P("fs", None, "tp"),
        P(("gr", "fs"), "tp"),
    )
    return jax.shard_map(
        per_device, mesh=mesh, in_specs=in_specs, out_specs=out_specs, check_vma=False
    )
```

```python
import jax
import jax.numpy as jnp
from jax import lax
from jax.experimental import pallas as pl
from jax.experimental.pallas import tpu as pltpu
from jax.sharding import PartitionSpec as P

MESH = pl.DeviceIdType.MESH
EPS = 1e-06
BF = jnp.bfloat16
F32 = jnp.float32

PLANES = ((0, 0, 0, 64), (1, 1, 0, 64), (2, -1, 0, 64), (3, 2, 0, 32), (3, -2, 32, 64))
TOK0, TOK1, HID0, HID1 = 0, 1, 2, 3
OWN_R0, OWN_R1, OWN_L0, OWN_L1, OWN_C, FAR_R, FAR_L, C_L, C_R, C_F0, C_F1 = range(11)


def kernel(
    prompt_hbm,
    gain_hbm,
    gate_hbm,
    up_hbm,
    down_hbm,
    routes_hbm,
    rw_hbm,
    w_gu0,
    w_gu1,
    w_d,
    hi1,
    lo1,
    acc,
    ansb,
    gain_ref,
    routes_ref,
    rw_ref,
    prompt_v,
    gate_v,
    up_v,
    down_v,
    stage_gu,
    stage_d,
    slots_x,
    tok,
    hid,
    dx,
    outs,
    ans,
    ansa,
    hi0,
    lo0,
    load_sem,
    wsend,
    wrecv,
    tsend,
    trecv,
    asend,
    arecv,
    dsend,
    drecv,
    rsend,
    rrecv,
):
    w_gu = (w_gu0, w_gu1)
    g = lax.axis_index("gr")
    f = lax.axis_index("fs")
    t = lax.axis_index("tp")
    me = g * 16 + f
    z = g * 4 + (f >> 2)
    y = f & 3
    x = t >> 1
    c = t & 1

    def at_zy(zz, yy):
        zz = (zz + 8) & 7
        yy = (yy + 4) & 3
        return zz >> 2, ((zz & 3) << 2) + yy

    right = (g, f, ((x + 1) & 3) * 2 + c)
    left = (g, f, ((x + 3) & 3) * 2 + c)
    other = (g, f, x * 2 + 1 - c)
    t_l = ((x + 3) & 3) * 2 + c
    t_r = ((x + 1) & 3) * 2 + c
    t_f = ((x + 2) & 3) * 2 + c

    barrier = pltpu.get_barrier_semaphore()

    def greet_zy(i, carry):
        gg, ff = at_zy(z + (i >> 2), y + (i & 3))
        pl.semaphore_signal(barrier, inc=1, device_id=(gg, ff, t), device_id_type=MESH)
        return carry

    lax.fori_loop(1, 32, greet_zy, 0)

    def greet_tp(i, carry):
        pl.semaphore_signal(barrier, inc=1, device_id=(g, f, (t + i) & 7), device_id_type=MESH)
        return carry

    lax.fori_loop(1, 8, greet_tp, 0)

    loads = [
        pltpu.make_async_copy(routes_hbm, routes_ref, load_sem.at[0]),
        pltpu.make_async_copy(prompt_hbm, prompt_v, load_sem.at[1]),
        pltpu.make_async_copy(gate_hbm, gate_v, load_sem.at[2]),
        pltpu.make_async_copy(up_hbm, up_v, load_sem.at[3]),
        pltpu.make_async_copy(down_hbm, down_v, load_sem.at[4]),
        pltpu.make_async_copy(gain_hbm, gain_ref, load_sem.at[5]),
        pltpu.make_async_copy(rw_hbm, rw_ref, load_sem.at[6]),
    ]
    for ld in loads:
        ld.start()

    def round_d(p):
        def body(i, carry):
            stage_d[p, i] = down_v[i, p].astype(BF)
            return carry

        lax.fori_loop(0, 16, body, 0)
        w_d[p, me] = stage_d[p, f]

    def round_gu(p, gain):
        def body(i, carry):
            stage_gu[p, i, :, 0:128] = (gain * gate_v[i, p]).astype(BF)
            stage_gu[p, i, :, 128:256] = (gain * up_v[i, p]).astype(BF)
            return carry

        lax.fori_loop(0, 16, body, 0)
        w_gu[p][me] = stage_gu[p, f]

    def send_w(stage, dest, sem, rows):
        def body(i, carry):
            gg, ff = at_zy(z + (i >> 2), y + (i & 3))
            pltpu.make_async_remote_copy(
                src_ref=stage.at[ff, rows],
                dst_ref=dest.at[me, rows],
                send_sem=wsend.at[sem],
                recv_sem=wrecv.at[sem],
                device_id=(gg, ff, t),
                device_id_type=MESH,
            ).start()
            return carry

        lax.fori_loop(1, 32, body, 0)

    def await_w(sems, dest, sem, rows):
        part = dest.at[pl.ds(0, 31), rows]
        pltpu.make_async_copy(part, part, sems.at[sem]).wait()

    def copy_to(ref, sems, i, where):
        return pltpu.make_async_remote_copy(
            src_ref=ref,
            dst_ref=ref,
            send_sem=asend.at[sems, i],
            recv_sem=arecv.at[sems, i],
            device_id=where,
            device_id_type=MESH,
        )

    def piece(kind, tt, half):
        p = kind % 2
        if kind < 2:
            ref = tok.at[p, tt]
            return ref if half is None else ref.at[pl.ds(8 * half, 8)]
        ref = hid.at[p, tt]
        return ref if half is None else ref.at[pl.ds(512 * half, 512)]

    def ag_own(kind):
        copy_to(piece(kind, t, 0), kind, OWN_R0, right).start()
        copy_to(piece(kind, t, 1), kind, OWN_L1, left).start()
        copy_to(piece(kind, t, 1), kind, OWN_R1, right).start()
        copy_to(piece(kind, t, 0), kind, OWN_L0, left).start()
        copy_to(piece(kind, t, None), kind, OWN_C, other).start()

    def ag_relay(kind):
        copy_to(piece(kind, t_l, 0), kind, OWN_R0, right).wait_recv()
        copy_to(piece(kind, t_l, 0), kind, FAR_R, right).start()
        copy_to(piece(kind, t_r, 1), kind, OWN_L1, left).wait_recv()
        copy_to(piece(kind, t_r, 1), kind, FAR_L, left).start()

    def ag_pass(kind):
        copy_to(piece(kind, t_l, 1), kind, OWN_R1, right).wait_recv()
        copy_to(piece(kind, t_l, None), kind, C_L, other).start()
        copy_to(piece(kind, t_r, 0), kind, OWN_L0, left).wait_recv()
        copy_to(piece(kind, t_r, None), kind, C_R, other).start()

    def ag_far(kind):
        copy_to(piece(kind, t_f, 0), kind, FAR_R, right).wait_recv()
        copy_to(piece(kind, t_f, 0), kind, C_F0, other).start()
        copy_to(piece(kind, t_f, 1), kind, FAR_L, left).wait_recv()
        copy_to(piece(kind, t_f, 1), kind, C_F1, other).start()

    def ag_end(kind):
        for i, half in ((OWN_C, None), (C_L, None), (C_R, None), (C_F0, 0), (C_F1, 1)):
            copy_to(piece(kind, t, half), kind, i, other).wait_recv()

    def ag_drain(kind):
        for i in (OWN_C, C_L, C_R):
            copy_to(piece(kind, t, None), kind, i, other).wait_send()
        for i in (OWN_R0, OWN_R1, OWN_L0, OWN_L1, FAR_R, FAR_L, C_F0, C_F1):
            copy_to(piece(kind, t, 0), kind, i, other).wait_send()

    def send_tokens(p):
        for j, dz, lo, hi in PLANES:
            for dy in range(4):
                gg, ff = at_zy(z + dz, y + dy)
                if dz == 0 and dy == 0:
                    continue
                pltpu.make_async_remote_copy(
                    src_ref=slots_x.at[p, ff, pl.ds(lo, hi - lo)],
                    dst_ref=tok.at[p, t, j * 4 + y, pl.ds(lo, hi - lo)],
                    send_sem=tsend.at[p],
                    recv_sem=trecv.at[p],
                    device_id=(gg, ff, t),
                    device_id_type=MESH,
                ).start()
        tok[p, t, y] = slots_x[p, f]

    def await_tokens(sems, p):
        part = slots_x.at[p, pl.ds(0, 15)]
        pltpu.make_async_copy(part, part, sems.at[p]).wait()

    def back(p, sem):
        return (ans, ansa, ansb)[sem]

    def send_back(p, plane, sem, lanes):
        for j, dz, lo, hi in PLANES:
            for dy in range(4):
                if j != plane or (dz == 0 and dy == 0):
                    continue
                gg, ff = at_zy(z - dz, y + dy)
                pltpu.make_async_remote_copy(
                    src_ref=outs.at[p, j * 4 + ((y + dy) & 3), pl.ds(lo, hi - lo), lanes],
                    dst_ref=back(p, sem).at[f, pl.ds(lo, hi - lo)],
                    send_sem=rsend.at[sem],
                    recv_sem=rrecv.at[sem],
                    device_id=(gg, ff, t),
                    device_id_type=MESH,
                ).start()
        if plane == 0:
            back(p, sem)[f] = outs[p, y, :, lanes]

    def await_back(sems, p, sem, lanes):
        part = outs.at[p, pl.ds(0, 15), :, lanes]
        pltpu.make_async_copy(part, part, sems.at[sem]).wait()

    def send_dx(p, h):
        def body(i, carry):
            tt = (t + i) & 7
            pltpu.make_async_remote_copy(
                src_ref=w_d.at[p, pl.ds(tt * 4, 4), pl.ds(32 * h, 32)],
                dst_ref=dx.at[p, h, t],
                send_sem=dsend.at[p, h],
                recv_sem=drecv.at[p, h],
                device_id=(g, f, tt),
                device_id_type=MESH,
            ).start()
            return carry

        lax.fori_loop(1, 8, body, 0)
        dx[p, h, t] = w_d[p, pl.ds(t * 4, 4), pl.ds(32 * h, 32)]

    def await_dx(sems, p, h):
        part = dx.at[p, h, pl.ds(0, 7)]
        pltpu.make_async_copy(part, part, sems.at[p, h]).wait()

    def hidden(p):
        def body(r, carry):
            rows = jnp.concatenate(
                [tok[p, tt, pl.ds(r * 4, 4)].reshape(256, 256) for tt in range(8)], axis=1
            )
            pre = jnp.dot(rows, w_gu[p][...].reshape(2048, 256), preferred_element_type=F32) * 2048 ** (-0.5)
            gate, up = pre[:, 0:128], pre[:, 128:256]
            value = gate / (1.0 + jnp.exp(-gate)) * up
            hid[p, t, pl.ds(r * 256, 256)] = value.astype(BF)
            return carry

        lax.fori_loop(0, 4, body, 0)

    def expert_out(p, halves, sem, lanes):
        for r in (3, 1, 2, 0):
            rows = jnp.concatenate([hid[p, tt, pl.ds(r * 256, 256)] for tt in range(8)], axis=1)
            cols = jnp.concatenate(
                [
                    jnp.concatenate([dx[p, h, tt].reshape(128, 128) for tt in range(8)], axis=1)
                    for h in halves
                ],
                axis=0,
            )
            value = lax.dot_general(rows, cols, (((1,), (1,)), ((), ())), preferred_element_type=F32)
            value = (value * 1024 ** (-0.5)).astype(BF)
            outs[p, pl.ds(r * 4, 4), :, lanes] = value.reshape(4, 64, 128 * len(halves))
            send_back(p, r, sem, lanes)

    def blend(p, sem, lanes):
        for r in range(2):
            rows = pl.ds(r * 256, 256)
            values = back(p, sem)[...].reshape(1024, lanes.size)
            part = jnp.dot((hi0, hi1)[p][rows], values, preferred_element_type=F32)
            part += jnp.dot((lo0, lo1)[p][rows], values, preferred_element_type=F32)
            if p == 0:
                acc[rows] = part
            else:
                acc[rows, lanes] += part

    whole = pl.ds(0, 256)
    low, high = pl.ds(0, 128), pl.ds(128, 128)
    all_rows = pl.ds(0, 64)
    rows_a, rows_b = pl.ds(0, 32), pl.ds(32, 32)

    loads[0].wait()
    row_i = lax.broadcasted_iota(jnp.int32, (512, 512), 0)
    col_i = lax.broadcasted_iota(jnp.int32, (512, 512), 1)
    diag = col_i == row_i

    def column(row):
        return jnp.sum(jnp.where(diag, row, 0.0), axis=1, keepdims=True)

    experts = lax.broadcasted_iota(jnp.int32, (32, 512), 0)
    hit0 = jnp.where(routes_ref[0:1] == experts, 1.0, 0.0)
    hit1 = jnp.where(routes_ref[1:2] == experts, 1.0, 0.0)
    before = jnp.where(row_i < col_i, 1.0, 0.0).astype(BF)
    rank0 = jnp.dot(hit0.astype(BF), before, preferred_element_type=F32)
    rank1 = jnp.dot(hit1.astype(BF), before, preferred_element_type=F32) + jnp.sum(hit0, axis=1, keepdims=True)
    place = ((experts >> 1) * 64 + (experts & 1) * 1024).astype(F32)
    slot0_row = jnp.sum((rank0 + place) * hit0, axis=0, keepdims=True)
    slot1_row = jnp.sum((rank1 + place) * hit1, axis=0, keepdims=True)

    loads[1].wait()
    wide = prompt_v[...].astype(F32)
    scale = lax.rsqrt(jnp.sum(wide * wide, axis=1, keepdims=True) * (1.0 / 2048) + EPS)
    mine = prompt_v[:, pl.ds(pl.multiple_of(t * 256, 256), 256)].astype(F32)
    normed = (mine * scale).astype(BF)

    def pick_slots(p):
        for r in range(4):
            number = (lax.broadcasted_iota(jnp.int32, (256, 512), 0) + (p * 1024 + r * 256)).astype(F32)
            pick = jnp.where((number == slot0_row) | (number == slot1_row), 1.0, 0.0).astype(BF)
            rows = jnp.dot(pick, normed, preferred_element_type=F32).astype(BF)
            slots_x[p, pl.ds(r * 4, 4)] = rows.reshape(4, 64, 256)

    pick_slots(0)
    pick_slots(1)
    loads[4].wait()
    round_d(0)
    pl.semaphore_wait(barrier, 38)
    send_tokens(0)
    send_tokens(1)
    loads[2].wait()
    loads[3].wait()
    loads[5].wait()
    eye = lax.broadcasted_iota(jnp.int32, (64, 64), 0) == lax.broadcasted_iota(jnp.int32, (64, 64), 1)
    gain = jnp.sum(jnp.where(eye, gain_ref[...], 0.0), axis=1, keepdims=True)
    round_gu(0, gain)
    send_w(stage_gu.at[0], w_gu0, 2, all_rows)
    round_gu(1, gain)
    send_w(stage_gu.at[1], w_gu1, 3, all_rows)
    send_w(stage_d.at[0], w_d.at[0], 0, all_rows)
    round_d(1)
    send_w(stage_d.at[1], w_d.at[1], 1, rows_a)
    send_w(stage_d.at[1], w_d.at[1], 4, rows_b)
    await_tokens(trecv, 0)
    ag_own(TOK0)
    await_tokens(trecv, 1)
    ag_own(TOK1)
    loads[6].wait()
    slot0 = column(slot0_row)
    slot1 = column(slot1_row)
    rw0 = column(rw_ref[0:1])
    rw1 = column(rw_ref[1:2])
    for p in range(2):
        for r in range(4):
            cols = pl.ds(r * 256, 256)
            number = (lax.broadcasted_iota(jnp.int32, (512, 256), 1) + (p * 1024 + r * 256)).astype(F32)
            weight = jnp.where(number == slot0, rw0, jnp.where(number == slot1, rw1, 0.0))
            upper = weight.astype(BF)
            (hi0, hi1)[p][:, cols] = upper
            (lo0, lo1)[p][:, cols] = (weight - upper.astype(F32)).astype(BF)
    ag_relay(TOK0)
    ag_pass(TOK0)
    ag_relay(TOK1)
    ag_far(TOK0)
    ag_pass(TOK1)
    ag_far(TOK1)
    ag_end(TOK0)
    await_w(wrecv, w_gu0, 2, all_rows)
    hidden(0)
    ag_own(HID0)
    ag_end(TOK1)
    ag_relay(HID0)
    ag_pass(HID0)
    ag_far(HID0)
    ag_end(HID0)
    await_w(wrecv, w_gu1, 3, all_rows)
    hidden(1)
    ag_own(HID1)
    ag_relay(HID1)
    ag_pass(HID1)
    await_w(wrecv, w_d.at[0], 0, all_rows)
    send_dx(0, 0)
    send_dx(0, 1)
    ag_far(HID1)
    ag_end(HID1)
    await_dx(drecv, 0, 0)
    await_w(wrecv, w_d.at[1], 1, rows_a)
    send_dx(1, 0)
    await_dx(drecv, 0, 1)
    expert_out(0, (0, 1), 0, whole)
    await_w(wrecv, w_d.at[1], 4, rows_b)
    send_dx(1, 1)
    await_dx(drecv, 1, 0)
    expert_out(1, (0,), 1, low)
    await_dx(drecv, 1, 1)
    expert_out(1, (1,), 2, high)
    for kind in range(4):
        ag_drain(kind)
    for p in range(2):
        await_tokens(tsend, p)
        for h in range(2):
            await_dx(dsend, p, h)
    await_w(wsend, w_d.at[0], 0, all_rows)
    await_w(wsend, w_d.at[1], 1, rows_a)
    await_w(wsend, w_gu0, 2, all_rows)
    await_w(wsend, w_gu1, 3, all_rows)
    await_w(wsend, w_d.at[1], 4, rows_b)
    await_back(rrecv, 0, 0, whole)
    blend(0, 0, whole)
    await_back(rsend, 0, 0, whole)
    await_back(rrecv, 1, 1, low)
    blend(1, 1, low)
    await_back(rsend, 1, 1, low)
    await_back(rsend, 1, 2, high)
    await_back(rrecv, 1, 2, high)


def copy_out(
    w_gu0,
    w_gu1,
    w_d,
    hi1,
    lo1,
    acc,
    ansb,
    gate_out,
    up_out,
    down_out,
    blend_out,
    blend_v,
    sem,
):
    copies = [
        pltpu.make_async_copy(w_gu0.at[:, :, pl.ds(0, 128)], gate_out.at[0], sem.at[0]),
        pltpu.make_async_copy(w_gu1.at[:, :, pl.ds(0, 128)], gate_out.at[1], sem.at[1]),
        pltpu.make_async_copy(w_gu0.at[:, :, pl.ds(128, 128)], up_out.at[0], sem.at[2]),
        pltpu.make_async_copy(w_gu1.at[:, :, pl.ds(128, 128)], up_out.at[1], sem.at[3]),
        pltpu.make_async_copy(w_d, down_out, sem.at[4]),
        pltpu.make_async_copy(blend_v, blend_out, sem.at[5]),
    ]
    for cp in copies[:5]:
        cp.start()
    a = lax.broadcasted_iota(jnp.int32, (256, 256), 0)
    b = lax.broadcasted_iota(jnp.int32, (256, 256), 1)
    goes = a == ((b >> 5) & 1) * 128 + (b >> 6) * 32 + (b & 31)
    to_place = jnp.where(goes, 1.0, 0.0).astype(BF)
    values = ansb[...].reshape(1024, 128)
    part = jnp.dot(hi1[...], values, preferred_element_type=F32)
    part += jnp.dot(lo1[...], values, preferred_element_type=F32)
    total = jnp.concatenate([acc[:, 0:128], acc[:, 128:256] + part], axis=1).astype(BF)
    blend_v[...] = jnp.dot(total, to_place, preferred_element_type=F32).astype(BF)
    copies[5].start()
    for cp in copies:
        cp.wait()


def per_device(prompt, norm_gain, gate_master, up_master, down_master, routes, route_weights):
    hbm = pl.BlockSpec(memory_space=pltpu.HBM)
    vmem = pl.BlockSpec(memory_space=pltpu.VMEM)
    ready = jax.ShapeDtypeStruct((2, 32, 64, 128), BF)
    both = jax.ShapeDtypeStruct((32, 64, 256), BF)
    block = jax.ShapeDtypeStruct((512, 256), BF)
    select = jax.ShapeDtypeStruct((512, 1024), BF)
    total = jax.ShapeDtypeStruct((512, 256), F32)
    part = jax.ShapeDtypeStruct((16, 64, 128), BF)
    dma = pltpu.SemaphoreType.DMA
    split = lambda a: a.reshape(16, 2, 64, 128)
    passed = pl.pallas_call(
        kernel,
        out_shape=(both, both, ready, select, select, total, part),
        in_specs=[hbm] * 7,
        out_specs=(vmem,) * 7,
        scratch_shapes=[
            pltpu.VMEM((1, 64), F32),
            pltpu.VMEM((2, 512), jnp.int32),
            pltpu.VMEM((2, 512), F32),
            pltpu.VMEM((512, 2048), BF),
            pltpu.VMEM((16, 2, 64, 128), F32),
            pltpu.VMEM((16, 2, 64, 128), F32),
            pltpu.VMEM((16, 2, 64, 128), F32),
            pltpu.VMEM((2, 16, 64, 256), BF),
            pltpu.VMEM((2, 16, 64, 128), BF),
            pltpu.VMEM((2, 16, 64, 256), BF),
            pltpu.VMEM((2, 8, 16, 64, 256), BF),
            pltpu.VMEM((2, 8, 1024, 128), BF),
            pltpu.VMEM((2, 2, 8, 4, 32, 128), BF),
            pltpu.VMEM((2, 16, 64, 256), BF),
            pltpu.VMEM((16, 64, 256), BF),
            pltpu.VMEM((16, 64, 128), BF),
            pltpu.VMEM((512, 1024), BF),
            pltpu.VMEM((512, 1024), BF),
            dma((7,)),
            dma((5,)),
            dma((5,)),
            dma((2,)),
            dma((2,)),
            dma((4, 11)),
            dma((4, 11)),
            dma((2, 2)),
            dma((2, 2)),
            dma((3,)),
            dma((3,)),
        ],
        compiler_params=pltpu.CompilerParams(
            collective_id=0, has_side_effects=True, vmem_limit_bytes=48 * 2**20
        ),
    )(
        *[
            pltpu.with_memory_space_constraint(a, pltpu.HBM)
            for a in (
                prompt,
                norm_gain.reshape(1, 64),
                split(gate_master),
                split(up_master),
                split(down_master),
                routes.T,
                route_weights.T,
            )
        ]
    )
    gate, up, down, out = pl.pallas_call(
        copy_out,
        out_shape=(ready, ready, ready, block),
        in_specs=[vmem] * 7,
        out_specs=(hbm,) * 4,
        scratch_shapes=[pltpu.VMEM((512, 256), BF), dma((6,))],
        compiler_params=pltpu.CompilerParams(vmem_limit_bytes=16 * 2**20),
    )(*passed)
    flat = lambda a: a.reshape(2, 2048, 128)
    return flat(gate), flat(up), flat(down), out


def solution(mesh):
    in_specs = (
        P(("gr", "fs"), None),
        P(("gr", "fs")),
        P(None, ("gr", "fs"), "tp"),
        P(None, ("gr", "fs"), "tp"),
        P(None, ("gr", "fs"), "tp"),
        P(("gr", "fs"), None),
        P(("gr", "fs"), None),
    )
    out_specs = (
        P("fs", None, "tp"),
        P("fs", None, "tp"),
        P("fs", None, "tp"),
        P(("gr", "fs"), "tp"),
    )
    return jax.shard_map(
        per_device, mesh=mesh, in_specs=in_specs, out_specs=out_specs, check_vma=False
    )
```

```python
import jax
import jax.numpy as jnp
from jax import lax
from jax.experimental import pallas as pl
from jax.experimental.pallas import tpu as pltpu
from jax.sharding import PartitionSpec as P

MESH = pl.DeviceIdType.MESH
EPS = 1e-06
BF = jnp.bfloat16
F32 = jnp.float32

PLANES = ((0, 0, 0, 64), (1, 1, 0, 64), (2, -1, 0, 64), (3, 2, 0, 32), (3, -2, 32, 64))
TOK0, TOK1, HID0, HID1 = 0, 1, 2, 3
OWN_R0, OWN_R1, OWN_L0, OWN_L1, OWN_C, FAR_R, FAR_L, C_L, C_R, C_F0, C_F1 = range(11)


def kernel(
    prompt_hbm,
    gain_hbm,
    gate_hbm,
    up_hbm,
    down_hbm,
    routes_hbm,
    rw_hbm,
    w_gu0,
    w_gu1,
    w_d,
    hi1,
    lo1,
    acc,
    ansb,
    gain_ref,
    routes_ref,
    rw_ref,
    prompt_v,
    gate_v,
    up_v,
    down_v,
    stage_gu,
    stage_d,
    slots_x,
    near_x,
    near_m,
    got_x,
    got_m,
    spread,
    tok,
    hid,
    dx,
    outs,
    ans,
    ansa,
    hi0,
    lo0,
    load_sem,
    wsend,
    wrecv,
    tsend,
    trecv,
    nsend,
    nrecv,
    asend,
    arecv,
    dsend,
    drecv,
    rsend,
    rrecv,
):
    w_gu = (w_gu0, w_gu1)
    g = lax.axis_index("gr")
    f = lax.axis_index("fs")
    t = lax.axis_index("tp")
    me = g * 16 + f
    z = g * 4 + (f >> 2)
    y = f & 3
    x = t >> 1
    c = t & 1

    def at_zy(zz, yy):
        zz = (zz + 8) & 7
        yy = (yy + 4) & 3
        return zz >> 2, ((zz & 3) << 2) + yy

    right = (g, f, ((x + 1) & 3) * 2 + c)
    left = (g, f, ((x + 3) & 3) * 2 + c)
    other = (g, f, x * 2 + 1 - c)
    t_l = ((x + 3) & 3) * 2 + c
    t_r = ((x + 1) & 3) * 2 + c
    t_f = ((x + 2) & 3) * 2 + c

    barrier = pltpu.get_barrier_semaphore()

    def greet_zy(i, carry):
        gg, ff = at_zy(z + (i >> 2), y + (i & 3))
        pl.semaphore_signal(barrier, inc=1, device_id=(gg, ff, t), device_id_type=MESH)
        return carry

    lax.fori_loop(1, 32, greet_zy, 0)

    def greet_tp(i, carry):
        pl.semaphore_signal(barrier, inc=1, device_id=(g, f, (t + i) & 7), device_id_type=MESH)
        return carry

    lax.fori_loop(1, 8, greet_tp, 0)

    loads = [
        pltpu.make_async_copy(routes_hbm, routes_ref, load_sem.at[0]),
        pltpu.make_async_copy(prompt_hbm, prompt_v, load_sem.at[1]),
        pltpu.make_async_copy(gate_hbm, gate_v, load_sem.at[2]),
        pltpu.make_async_copy(up_hbm, up_v, load_sem.at[3]),
        pltpu.make_async_copy(down_hbm, down_v, load_sem.at[4]),
        pltpu.make_async_copy(gain_hbm, gain_ref, load_sem.at[5]),
        pltpu.make_async_copy(rw_hbm, rw_ref, load_sem.at[6]),
    ]
    for ld in loads:
        ld.start()

    def round_d(p):
        def body(i, carry):
            stage_d[p, i] = down_v[i, p].astype(BF)
            return carry

        lax.fori_loop(0, 16, body, 0)
        w_d[p, me] = stage_d[p, f]

    def round_gu(p, gain):
        def body(i, carry):
            stage_gu[p, i, :, 0:128] = (gain * gate_v[i, p]).astype(BF)
            stage_gu[p, i, :, 128:256] = (gain * up_v[i, p]).astype(BF)
            return carry

        lax.fori_loop(0, 16, body, 0)
        w_gu[p][me] = stage_gu[p, f]

    def send_w(stage, dest, sem, rows, first=1, last=32, step=1):
        def body(n, carry):
            i = n * step
            gg, ff = at_zy(z + (i >> 2), y + (i & 3))
            pltpu.make_async_remote_copy(
                src_ref=stage.at[ff, rows],
                dst_ref=dest.at[me, rows],
                send_sem=wsend.at[sem],
                recv_sem=wrecv.at[sem],
                device_id=(gg, ff, t),
                device_id_type=MESH,
            ).start()
            return carry

        lax.fori_loop(first, last, body, 0)

    def send_w_other(stage, dest, sem):
        def body(n, carry):
            i = n + n // 3 + 1
            gg, ff = at_zy(z + (i >> 2), y + (i & 3))
            pltpu.make_async_remote_copy(
                src_ref=stage.at[ff],
                dst_ref=dest.at[me],
                send_sem=wsend.at[sem],
                recv_sem=wrecv.at[sem],
                device_id=(gg, ff, t),
                device_id_type=MESH,
            ).start()
            return carry

        lax.fori_loop(0, 24, body, 0)

    def await_w(sems, dest, sem, rows):
        part = dest.at[pl.ds(0, 31), rows]
        pltpu.make_async_copy(part, part, sems.at[sem]).wait()

    def copy_to(ref, sems, i, where):
        return pltpu.make_async_remote_copy(
            src_ref=ref,
            dst_ref=ref,
            send_sem=asend.at[sems, i],
            recv_sem=arecv.at[sems, i],
            device_id=where,
            device_id_type=MESH,
        )

    def piece(kind, tt, half):
        p = kind % 2
        if kind < 2:
            ref = tok.at[p, tt]
            return ref if half is None else ref.at[pl.ds(8 * half, 8)]
        ref = hid.at[p, tt]
        return ref if half is None else ref.at[pl.ds(512 * half, 512)]

    def ag_own(kind):
        copy_to(piece(kind, t, 0), kind, OWN_R0, right).start()
        copy_to(piece(kind, t, 1), kind, OWN_L1, left).start()
        copy_to(piece(kind, t, 1), kind, OWN_R1, right).start()
        copy_to(piece(kind, t, 0), kind, OWN_L0, left).start()
        copy_to(piece(kind, t, None), kind, OWN_C, other).start()

    def ag_relay(kind):
        copy_to(piece(kind, t_l, 0), kind, OWN_R0, right).wait_recv()
        copy_to(piece(kind, t_l, 0), kind, FAR_R, right).start()
        copy_to(piece(kind, t_r, 1), kind, OWN_L1, left).wait_recv()
        copy_to(piece(kind, t_r, 1), kind, FAR_L, left).start()

    def ag_pass(kind):
        copy_to(piece(kind, t_l, 1), kind, OWN_R1, right).wait_recv()
        copy_to(piece(kind, t_l, None), kind, C_L, other).start()
        copy_to(piece(kind, t_r, 0), kind, OWN_L0, left).wait_recv()
        copy_to(piece(kind, t_r, None), kind, C_R, other).start()

    def ag_far(kind):
        copy_to(piece(kind, t_f, 0), kind, FAR_R, right).wait_recv()
        copy_to(piece(kind, t_f, 0), kind, C_F0, other).start()
        copy_to(piece(kind, t_f, 1), kind, FAR_L, left).wait_recv()
        copy_to(piece(kind, t_f, 1), kind, C_F1, other).start()

    def ag_end(kind):
        for i, half in ((OWN_C, None), (C_L, None), (C_R, None), (C_F0, 0), (C_F1, 1)):
            copy_to(piece(kind, t, half), kind, i, other).wait_recv()

    def ag_drain(kind):
        for i in (OWN_C, C_L, C_R):
            copy_to(piece(kind, t, None), kind, i, other).wait_send()
        for i in (OWN_R0, OWN_R1, OWN_L0, OWN_L1, FAR_R, FAR_L, C_F0, C_F1):
            copy_to(piece(kind, t, 0), kind, i, other).wait_send()

    def send_tokens(p):
        for j, dz, lo, hi in PLANES:
            for dy in range(4):
                if j in (1, 2) or (dz == 0 and dy == 0):
                    continue
                gg, ff = at_zy(z + dz, y + dy)
                pltpu.make_async_remote_copy(
                    src_ref=slots_x.at[p, j // 3, (y + dy) & 3, pl.ds(lo, hi - lo)],
                    dst_ref=tok.at[p, t, j * 4 + y, pl.ds(lo, hi - lo)],
                    send_sem=tsend.at[p],
                    recv_sem=trecv.at[p],
                    device_id=(gg, ff, t),
                    device_id_type=MESH,
                ).start()
        tok[p, t, y] = slots_x[p, 0, y]

    def near_copies(d):
        gg, ff = at_zy(z + 1 - 2 * d, y)
        return [
            pltpu.make_async_remote_copy(
                src_ref=src.at[d],
                dst_ref=dst.at[d],
                send_sem=nsend.at[d, i],
                recv_sem=nrecv.at[d, i],
                device_id=(gg, ff, t),
                device_id_type=MESH,
            )
            for i, (src, dst) in enumerate(((near_x, got_x), (near_m, got_m)))
        ]

    def pass_near(d):
        for cp in near_copies(d):
            cp.wait_recv()
        for p in range(2):
            number = (lax.broadcasted_iota(jnp.int32, (256, 256), 0) + p * 256).astype(F32)
            pick = (number == got_m[d, 0:1]) | (number == got_m[d, 1:2])
            rows = jnp.dot(jnp.where(pick, 1.0, 0.0).astype(BF), got_x[d], preferred_element_type=F32)
            spread[d, p] = rows.astype(BF).reshape(4, 64, 256)
            for dy in (2, 1, 3):
                gg, ff = at_zy(z, y + dy)
                pltpu.make_async_remote_copy(
                    src_ref=spread.at[d, p, (y + dy) & 3],
                    dst_ref=tok.at[p, t, (d + 1) * 4 + y],
                    send_sem=tsend.at[p],
                    recv_sem=trecv.at[p],
                    device_id=(gg, ff, t),
                    device_id_type=MESH,
                ).start()
            tok[p, t, (d + 1) * 4 + y] = spread[d, p, y]

    def await_tokens(sems, p):
        part = tok.at[p, t, pl.ds(0, 13)]
        pltpu.make_async_copy(part, part, sems.at[p]).wait()

    def back(p, sem):
        return (ans, ansa, ansb)[sem]

    def send_back(p, plane, sem, lanes):
        for j, dz, lo, hi in PLANES:
            for dy in range(4):
                if j != plane or (dz == 0 and dy == 0):
                    continue
                gg, ff = at_zy(z - dz, y + dy)
                pltpu.make_async_remote_copy(
                    src_ref=outs.at[p, j * 4 + ((y + dy) & 3), pl.ds(lo, hi - lo), lanes],
                    dst_ref=back(p, sem).at[f, pl.ds(lo, hi - lo)],
                    send_sem=rsend.at[sem],
                    recv_sem=rrecv.at[sem],
                    device_id=(gg, ff, t),
                    device_id_type=MESH,
                ).start()
        if plane == 0:
            back(p, sem)[f] = outs[p, y, :, lanes]

    def await_back(sems, p, sem, lanes):
        part = outs.at[p, pl.ds(0, 15), :, lanes]
        pltpu.make_async_copy(part, part, sems.at[sem]).wait()

    def send_dx(p, h):
        def body(i, carry):
            tt = (t + i) & 7
            pltpu.make_async_remote_copy(
                src_ref=w_d.at[p, pl.ds(tt * 4, 4), pl.ds(32 * h, 32)],
                dst_ref=dx.at[p, h, t],
                send_sem=dsend.at[p, h],
                recv_sem=drecv.at[p, h],
                device_id=(g, f, tt),
                device_id_type=MESH,
            ).start()
            return carry

        lax.fori_loop(1, 8, body, 0)
        dx[p, h, t] = w_d[p, pl.ds(t * 4, 4), pl.ds(32 * h, 32)]

    def await_dx(sems, p, h):
        part = dx.at[p, h, pl.ds(0, 7)]
        pltpu.make_async_copy(part, part, sems.at[p, h]).wait()

    def hidden(p):
        def body(r, carry):
            rows = jnp.concatenate(
                [tok[p, tt, pl.ds(r * 4, 4)].reshape(256, 256) for tt in range(8)], axis=1
            )
            pre = jnp.dot(rows, w_gu[p][...].reshape(2048, 256), preferred_element_type=F32) * 2048 ** (-0.5)
            gate, up = pre[:, 0:128], pre[:, 128:256]
            value = gate / (1.0 + jnp.exp(-gate)) * up
            hid[p, t, pl.ds(r * 256, 256)] = value.astype(BF)
            return carry

        lax.fori_loop(0, 4, body, 0)

    def expert_out(p, halves, sem, lanes):
        for r in (3, 1, 2, 0):
            rows = jnp.concatenate([hid[p, tt, pl.ds(r * 256, 256)] for tt in range(8)], axis=1)
            cols = jnp.concatenate(
                [
                    jnp.concatenate([dx[p, h, tt].reshape(128, 128) for tt in range(8)], axis=1)
                    for h in halves
                ],
                axis=0,
            )
            value = lax.dot_general(rows, cols, (((1,), (1,)), ((), ())), preferred_element_type=F32)
            value = (value * 1024 ** (-0.5)).astype(BF)
            outs[p, pl.ds(r * 4, 4), :, lanes] = value.reshape(4, 64, 128 * len(halves))
            send_back(p, r, sem, lanes)

    def blend(p, sem, lanes):
        for r in range(2):
            rows = pl.ds(r * 256, 256)
            values = back(p, sem)[...].reshape(1024, lanes.size)
            part = jnp.dot((hi0, hi1)[p][rows], values, preferred_element_type=F32)
            part += jnp.dot((lo0, lo1)[p][rows], values, preferred_element_type=F32)
            if p == 0:
                acc[rows] = part
            else:
                acc[rows, lanes] += part

    whole = pl.ds(0, 256)
    low, high = pl.ds(0, 128), pl.ds(128, 128)
    all_rows = pl.ds(0, 64)
    rows_a, rows_b = pl.ds(0, 32), pl.ds(32, 32)

    loads[0].wait()
    row_i = lax.broadcasted_iota(jnp.int32, (512, 512), 0)
    col_i = lax.broadcasted_iota(jnp.int32, (512, 512), 1)
    diag = col_i == row_i

    def column(row):
        return jnp.sum(jnp.where(diag, row, 0.0), axis=1, keepdims=True)

    experts = lax.broadcasted_iota(jnp.int32, (32, 512), 0)
    hit0 = jnp.where(routes_ref[0:1] == experts, 1.0, 0.0)
    hit1 = jnp.where(routes_ref[1:2] == experts, 1.0, 0.0)
    before = jnp.where(row_i < col_i, 1.0, 0.0).astype(BF)
    rank0 = jnp.dot(hit0.astype(BF), before, preferred_element_type=F32)
    rank1 = jnp.dot(hit1.astype(BF), before, preferred_element_type=F32) + jnp.sum(hit0, axis=1, keepdims=True)
    place = ((experts >> 1) * 64 + (experts & 1) * 1024).astype(F32)
    slot0_row = jnp.sum((rank0 + place) * hit0, axis=0, keepdims=True)
    slot1_row = jnp.sum((rank1 + place) * hit1, axis=0, keepdims=True)

    loads[1].wait()
    wide = prompt_v[...].astype(F32)
    scale = lax.rsqrt(jnp.sum(wide * wide, axis=1, keepdims=True) * (1.0 / 2048) + EPS)
    mine = prompt_v[:, pl.ds(pl.multiple_of(t * 256, 256), 256)].astype(F32)
    normed = (mine * scale).astype(BF)

    def group_of(dz):
        return ((z + dz) & 3).astype(F32)

    numbers = lax.broadcasted_iota(jnp.int32, (256, 512), 0).astype(F32)

    def pick_slots(p):
        for j in range(2):
            number = numbers + (group_of(2 * j) * 256.0 + p * 1024.0)
            pick = jnp.where((number == slot0_row) | (number == slot1_row), 1.0, 0.0).astype(BF)
            rows = jnp.dot(pick, normed, preferred_element_type=F32).astype(BF)
            slots_x[p, j] = rows.reshape(4, 64, 256)

    def along(values, hit):
        return jnp.sum(values.astype(F32) * hit, axis=0, keepdims=True)

    group_row = along(experts >> 3, hit0)
    groups = lax.broadcasted_iota(jnp.int32, (8, 512), 0).astype(F32)
    group_hit = jnp.where(groups == group_row, 1.0, 0.0)
    group_rank = jnp.dot(group_hit.astype(BF), before, preferred_element_type=F32)
    number_row = along(group_rank, group_hit) + group_row * 256.0
    facts = (
        along(experts & 1, hit0),
        along((experts >> 1) & 3, hit0),
        along(rank0, hit0),
        along(experts & 1, hit1),
        along((experts >> 1) & 3, hit1),
        along(rank1, hit1),
        jnp.ones((1, 512), F32),
        jnp.zeros((1, 512), F32),
    )
    facts = jnp.concatenate(facts, axis=0).astype(BF)
    for d in range(2):
        pick = jnp.where(numbers + group_of(1 - 2 * d) * 256.0 == number_row, 1.0, 0.0).astype(BF)
        near_x[d] = jnp.dot(pick, normed, preferred_element_type=F32).astype(BF)
        m = lax.dot_general(facts, pick, (((1,), (1,)), ((), ())), preferred_element_type=F32)
        first = m[0:1] * 256.0 + m[1:2] * 64.0 + m[2:3] + (m[6:7] - 1.0)
        second = m[3:4] * 256.0 + m[4:5] * 64.0 + m[5:6] + (m[6:7] - 1.0)
        near_m[d] = jnp.concatenate([first, second, m[2:8]], axis=0)
    pick_slots(0)
    pick_slots(1)
    loads[4].wait()
    round_d(0)
    pl.semaphore_wait(barrier, 38)
    for d in range(2):
        for cp in near_copies(d):
            cp.start()
    send_tokens(0)
    send_tokens(1)
    loads[2].wait()
    loads[3].wait()
    loads[5].wait()
    eye = lax.broadcasted_iota(jnp.int32, (64, 64), 0) == lax.broadcasted_iota(jnp.int32, (64, 64), 1)
    gain = jnp.sum(jnp.where(eye, gain_ref[...], 0.0), axis=1, keepdims=True)
    round_gu(0, gain)
    send_w(stage_gu.at[0], w_gu0, 2, all_rows, 1, 8, 4)
    round_gu(1, gain)
    pass_near(0)
    pass_near(1)
    send_w_other(stage_gu.at[0], w_gu0, 2)
    send_w(stage_gu.at[1], w_gu1, 3, all_rows)
    send_w(stage_d.at[0], w_d.at[0], 0, all_rows)
    round_d(1)
    send_w(stage_d.at[1], w_d.at[1], 1, rows_a)
    send_w(stage_d.at[1], w_d.at[1], 4, rows_b)
    await_tokens(trecv, 0)
    ag_own(TOK0)
    await_tokens(trecv, 1)
    ag_own(TOK1)
    loads[6].wait()
    slot0 = column(slot0_row)
    slot1 = column(slot1_row)
    rw0 = column(rw_ref[0:1])
    rw1 = column(rw_ref[1:2])
    for p in range(2):
        for r in range(4):
            cols = pl.ds(r * 256, 256)
            number = (lax.broadcasted_iota(jnp.int32, (512, 256), 1) + (p * 1024 + r * 256)).astype(F32)
            weight = jnp.where(number == slot0, rw0, jnp.where(number == slot1, rw1, 0.0))
            upper = weight.astype(BF)
            (hi0, hi1)[p][:, cols] = upper
            (lo0, lo1)[p][:, cols] = (weight - upper.astype(F32)).astype(BF)
    ag_relay(TOK0)
    ag_pass(TOK0)
    ag_relay(TOK1)
    ag_far(TOK0)
    ag_pass(TOK1)
    ag_far(TOK1)
    ag_end(TOK0)
    await_w(wrecv, w_gu0, 2, all_rows)
    hidden(0)
    ag_own(HID0)
    ag_end(TOK1)
    ag_relay(HID0)
    ag_pass(HID0)
    ag_far(HID0)
    ag_end(HID0)
    await_w(wrecv, w_gu1, 3, all_rows)
    hidden(1)
    ag_own(HID1)
    ag_relay(HID1)
    ag_pass(HID1)
    await_w(wrecv, w_d.at[0], 0, all_rows)
    send_dx(0, 0)
    send_dx(0, 1)
    ag_far(HID1)
    ag_end(HID1)
    await_dx(drecv, 0, 0)
    await_w(wrecv, w_d.at[1], 1, rows_a)
    send_dx(1, 0)
    await_dx(drecv, 0, 1)
    expert_out(0, (0, 1), 0, whole)
    await_w(wrecv, w_d.at[1], 4, rows_b)
    send_dx(1, 1)
    await_dx(drecv, 1, 0)
    expert_out(1, (0,), 1, low)
    await_dx(drecv, 1, 1)
    expert_out(1, (1,), 2, high)
    for kind in range(4):
        ag_drain(kind)
    for d in range(2):
        for cp in near_copies(d):
            cp.wait_send()
    for p in range(2):
        await_tokens(tsend, p)
        for h in range(2):
            await_dx(dsend, p, h)
    await_w(wsend, w_d.at[0], 0, all_rows)
    await_w(wsend, w_d.at[1], 1, rows_a)
    await_w(wsend, w_gu0, 2, all_rows)
    await_w(wsend, w_gu1, 3, all_rows)
    await_w(wsend, w_d.at[1], 4, rows_b)
    await_back(rrecv, 0, 0, whole)
    blend(0, 0, whole)
    await_back(rsend, 0, 0, whole)
    await_back(rrecv, 1, 1, low)
    blend(1, 1, low)
    await_back(rsend, 1, 1, low)
    await_back(rsend, 1, 2, high)
    await_back(rrecv, 1, 2, high)


def copy_out(
    w_gu0,
    w_gu1,
    w_d,
    hi1,
    lo1,
    acc,
    ansb,
    gate_out,
    up_out,
    down_out,
    blend_out,
    blend_v,
    sem,
):
    copies = [
        pltpu.make_async_copy(w_gu0.at[:, :, pl.ds(0, 128)], gate_out.at[0], sem.at[0]),
        pltpu.make_async_copy(w_gu1.at[:, :, pl.ds(0, 128)], gate_out.at[1], sem.at[1]),
        pltpu.make_async_copy(w_gu0.at[:, :, pl.ds(128, 128)], up_out.at[0], sem.at[2]),
        pltpu.make_async_copy(w_gu1.at[:, :, pl.ds(128, 128)], up_out.at[1], sem.at[3]),
        pltpu.make_async_copy(w_d, down_out, sem.at[4]),
        pltpu.make_async_copy(blend_v, blend_out, sem.at[5]),
    ]
    for cp in copies[:5]:
        cp.start()
    a = lax.broadcasted_iota(jnp.int32, (256, 256), 0)
    b = lax.broadcasted_iota(jnp.int32, (256, 256), 1)
    goes = a == ((b >> 5) & 1) * 128 + (b >> 6) * 32 + (b & 31)
    to_place = jnp.where(goes, 1.0, 0.0).astype(BF)
    values = ansb[...].reshape(1024, 128)
    part = jnp.dot(hi1[...], values, preferred_element_type=F32)
    part += jnp.dot(lo1[...], values, preferred_element_type=F32)
    total = jnp.concatenate([acc[:, 0:128], acc[:, 128:256] + part], axis=1).astype(BF)
    blend_v[...] = jnp.dot(total, to_place, preferred_element_type=F32).astype(BF)
    copies[5].start()
    for cp in copies:
        cp.wait()


def per_device(prompt, norm_gain, gate_master, up_master, down_master, routes, route_weights):
    hbm = pl.BlockSpec(memory_space=pltpu.HBM)
    vmem = pl.BlockSpec(memory_space=pltpu.VMEM)
    ready = jax.ShapeDtypeStruct((2, 32, 64, 128), BF)
    both = jax.ShapeDtypeStruct((32, 64, 256), BF)
    block = jax.ShapeDtypeStruct((512, 256), BF)
    select = jax.ShapeDtypeStruct((512, 1024), BF)
    total = jax.ShapeDtypeStruct((512, 256), F32)
    part = jax.ShapeDtypeStruct((16, 64, 128), BF)
    dma = pltpu.SemaphoreType.DMA
    split = lambda a: a.reshape(16, 2, 64, 128)
    passed = pl.pallas_call(
        kernel,
        out_shape=(both, both, ready, select, select, total, part),
        in_specs=[hbm] * 7,
        out_specs=(vmem,) * 7,
        scratch_shapes=[
            pltpu.VMEM((1, 64), F32),
            pltpu.VMEM((2, 512), jnp.int32),
            pltpu.VMEM((2, 512), F32),
            pltpu.VMEM((512, 2048), BF),
            pltpu.VMEM((16, 2, 64, 128), F32),
            pltpu.VMEM((16, 2, 64, 128), F32),
            pltpu.VMEM((16, 2, 64, 128), F32),
            pltpu.VMEM((2, 16, 64, 256), BF),
            pltpu.VMEM((2, 16, 64, 128), BF),
            pltpu.VMEM((2, 2, 4, 64, 256), BF),
            pltpu.VMEM((2, 256, 256), BF),
            pltpu.VMEM((2, 8, 256), F32),
            pltpu.VMEM((2, 256, 256), BF),
            pltpu.VMEM((2, 8, 256), F32),
            pltpu.VMEM((2, 2, 4, 64, 256), BF),
            pltpu.VMEM((2, 8, 16, 64, 256), BF),
            pltpu.VMEM((2, 8, 1024, 128), BF),
            pltpu.VMEM((2, 2, 8, 4, 32, 128), BF),
            pltpu.VMEM((2, 16, 64, 256), BF),
            pltpu.VMEM((16, 64, 256), BF),
            pltpu.VMEM((16, 64, 128), BF),
            pltpu.VMEM((512, 1024), BF),
            pltpu.VMEM((512, 1024), BF),
            dma((7,)),
            dma((5,)),
            dma((5,)),
            dma((2,)),
            dma((2,)),
            dma((2, 2)),
            dma((2, 2)),
            dma((4, 11)),
            dma((4, 11)),
            dma((2, 2)),
            dma((2, 2)),
            dma((3,)),
            dma((3,)),
        ],
        compiler_params=pltpu.CompilerParams(
            collective_id=0, has_side_effects=True, vmem_limit_bytes=48 * 2**20
        ),
    )(
        *[
            pltpu.with_memory_space_constraint(a, pltpu.HBM)
            for a in (
                prompt,
                norm_gain.reshape(1, 64),
                split(gate_master),
                split(up_master),
                split(down_master),
                routes.T,
                route_weights.T,
            )
        ]
    )
    gate, up, down, out = pl.pallas_call(
        copy_out,
        out_shape=(ready, ready, ready, block),
        in_specs=[vmem] * 7,
        out_specs=(hbm,) * 4,
        scratch_shapes=[pltpu.VMEM((512, 256), BF), dma((6,))],
        compiler_params=pltpu.CompilerParams(vmem_limit_bytes=16 * 2**20),
    )(*passed)
    flat = lambda a: a.reshape(2, 2048, 128)
    return flat(gate), flat(up), flat(down), out


def solution(mesh):
    in_specs = (
        P(("gr", "fs"), None),
        P(("gr", "fs")),
        P(None, ("gr", "fs"), "tp"),
        P(None, ("gr", "fs"), "tp"),
        P(None, ("gr", "fs"), "tp"),
        P(("gr", "fs"), None),
        P(("gr", "fs"), None),
    )
    out_specs = (
        P("fs", None, "tp"),
        P("fs", None, "tp"),
        P("fs", None, "tp"),
        P(("gr", "fs"), "tp"),
    )
    return jax.shard_map(
        per_device, mesh=mesh, in_specs=in_specs, out_specs=out_specs, check_vma=False
    )
```

```python
import jax
import jax.numpy as jnp
from jax import lax
from jax.experimental import pallas as pl
from jax.experimental.pallas import tpu as pltpu
from jax.sharding import PartitionSpec as P

MESH = pl.DeviceIdType.MESH
EPS = 1e-06
BF = jnp.bfloat16
F32 = jnp.float32

PLANES = ((0, 0, 0, 64), (1, 2, 0, 32), (1, -2, 32, 64), (2, 1, 0, 64), (3, -1, 0, 64))
TOK0, TOK1, HID0, HID1 = 0, 1, 2, 3
TO_R, TO_L, TO_L2, FAR_R, FAR_L, ACROSS = 0, 3, 4, 5, 6, 7
PIECES = ((0, 4), (4, 4), (8, 8), (0, 8), (0, 16))
FIRST, WHOLE = 3, 4


def kernel(
    prompt_hbm,
    gain_hbm,
    gate_hbm,
    up_hbm,
    down_hbm,
    routes_hbm,
    rw_hbm,
    w_gu0,
    w_gu1,
    w_d,
    hi1,
    lo1,
    acc,
    ansb,
    gain_ref,
    routes_ref,
    rw_ref,
    prompt_v,
    gate_v,
    up_v,
    down_v,
    stage_gu,
    stage_d,
    slots_x,
    near_x,
    near_m,
    got_x,
    got_m,
    spread,
    tok,
    hid,
    dx,
    outs,
    ans,
    ansa,
    hi0,
    lo0,
    load_sem,
    wsend,
    wrecv,
    tsend,
    trecv,
    nsend,
    nrecv,
    asend,
    arecv,
    dsend,
    drecv,
    rsend,
    rrecv,
):
    w_gu = (w_gu0, w_gu1)
    g = lax.axis_index("gr")
    f = lax.axis_index("fs")
    t = lax.axis_index("tp")
    me = g * 16 + f
    z = g * 4 + (f >> 2)
    y = f & 3
    x = t >> 1
    c = t & 1

    def at_zy(zz, yy):
        zz = (zz + 8) & 7
        yy = (yy + 4) & 3
        return zz >> 2, ((zz & 3) << 2) + yy

    right = (g, f, ((x + 1) & 3) * 2 + c)
    left = (g, f, ((x + 3) & 3) * 2 + c)
    other = (g, f, x * 2 + 1 - c)
    t_l = ((x + 3) & 3) * 2 + c
    t_r = ((x + 1) & 3) * 2 + c
    t_f = ((x + 2) & 3) * 2 + c

    barrier = pltpu.get_barrier_semaphore()

    def greet_zy(i, carry):
        gg, ff = at_zy(z + (i >> 2), y + (i & 3))
        pl.semaphore_signal(barrier, inc=1, device_id=(gg, ff, t), device_id_type=MESH)
        return carry

    lax.fori_loop(1, 32, greet_zy, 0)

    def greet_tp(i, carry):
        pl.semaphore_signal(barrier, inc=1, device_id=(g, f, (t + i) & 7), device_id_type=MESH)
        return carry

    lax.fori_loop(1, 8, greet_tp, 0)

    loads = [
        pltpu.make_async_copy(routes_hbm, routes_ref, load_sem.at[0]),
        pltpu.make_async_copy(prompt_hbm, prompt_v, load_sem.at[1]),
        pltpu.make_async_copy(gate_hbm, gate_v, load_sem.at[2]),
        pltpu.make_async_copy(up_hbm, up_v, load_sem.at[3]),
        pltpu.make_async_copy(down_hbm, down_v, load_sem.at[4]),
        pltpu.make_async_copy(gain_hbm, gain_ref, load_sem.at[5]),
        pltpu.make_async_copy(rw_hbm, rw_ref, load_sem.at[6]),
    ]
    for ld in loads:
        ld.start()

    def round_d(p):
        def body(i, carry):
            stage_d[p, i] = down_v[i, p].astype(BF)
            return carry

        lax.fori_loop(0, 16, body, 0)
        w_d[p, me] = stage_d[p, f]

    def round_gu(p, gain):
        def body(i, carry):
            stage_gu[p, i, :, 0:128] = (gain * gate_v[i, p]).astype(BF)
            stage_gu[p, i, :, 128:256] = (gain * up_v[i, p]).astype(BF)
            return carry

        lax.fori_loop(0, 16, body, 0)
        w_gu[p][me] = stage_gu[p, f]

    def send_w(stage, dest, sem, rows, first=1, last=32, step=1):
        def body(n, carry):
            i = n * step
            gg, ff = at_zy(z + (i >> 2), y + (i & 3))
            pltpu.make_async_remote_copy(
                src_ref=stage.at[ff, rows],
                dst_ref=dest.at[me, rows],
                send_sem=wsend.at[sem],
                recv_sem=wrecv.at[sem],
                device_id=(gg, ff, t),
                device_id_type=MESH,
            ).start()
            return carry

        lax.fori_loop(first, last, body, 0)

    def send_w_other(stage, dest, sem):
        def body(n, carry):
            i = n + n // 3 + 1
            gg, ff = at_zy(z + (i >> 2), y + (i & 3))
            pltpu.make_async_remote_copy(
                src_ref=stage.at[ff],
                dst_ref=dest.at[me],
                send_sem=wsend.at[sem],
                recv_sem=wrecv.at[sem],
                device_id=(gg, ff, t),
                device_id_type=MESH,
            ).start()
            return carry

        lax.fori_loop(0, 24, body, 0)

    def await_w(sems, dest, sem, rows):
        part = dest.at[pl.ds(0, 31), rows]
        pltpu.make_async_copy(part, part, sems.at[sem]).wait()

    def copy_to(ref, sems, i, where):
        return pltpu.make_async_remote_copy(
            src_ref=ref,
            dst_ref=ref,
            send_sem=asend.at[sems],
            recv_sem=arecv.at[sems, i],
            device_id=where,
            device_id_type=MESH,
        )

    def piece(kind, tt, part):
        lo, size = PIECES[part]
        if kind < 2:
            return tok.at[kind, tt, pl.ds(lo, size)]
        return hid.at[kind - 2, tt, pl.ds(64 * lo, 64 * size)]

    def own_right(kind, part):
        copy_to(piece(kind, t, part), kind, TO_R + part, right).start()

    def own_left(kind, part):
        copy_to(piece(kind, t, part), kind, TO_L2 if part == 2 else TO_L, left).start()

    def own_other(kind):
        copy_to(piece(kind, t, WHOLE), kind, ACROSS, other).start()

    def relay_right(kind, part):
        copy_to(piece(kind, t_l, part), kind, TO_R + part, right).wait_recv()
        copy_to(piece(kind, t_l, part), kind, FAR_R, right).start()

    def relay_left(kind):
        copy_to(piece(kind, t_r, 2), kind, TO_L2, left).wait_recv()
        copy_to(piece(kind, t_r, 2), kind, FAR_L, left).start()

    def ag_pass(kind):
        copy_to(piece(kind, t_l, 2), kind, TO_R + 2, right).wait_recv()
        copy_to(piece(kind, t_l, WHOLE), kind, ACROSS, other).start()
        copy_to(piece(kind, t_r, FIRST), kind, TO_L, left).wait_recv()
        copy_to(piece(kind, t_r, WHOLE), kind, ACROSS, other).start()

    def ag_far(kind):
        copy_to(piece(kind, t_f, FIRST), kind, FAR_R, right).wait_recv()
        copy_to(piece(kind, t_f, FIRST), kind, ACROSS, other).start()
        copy_to(piece(kind, t_f, 2), kind, FAR_L, left).wait_recv()
        copy_to(piece(kind, t_f, 2), kind, ACROSS, other).start()

    def slices(kind, count):
        return (tok, tok, hid, hid)[kind].at[kind & 1, pl.ds(0, count)]

    def ag_end(kind):
        ref = slices(kind, 4)
        pltpu.make_async_copy(ref, ref, arecv.at[kind, ACROSS]).wait()

    def ag_drain(kind):
        ref = slices(kind, 7)
        pltpu.make_async_copy(ref, ref, asend.at[kind]).wait()

    def send_tokens(p):
        for j, dz, lo, hi in PLANES:
            for dy in range(4):
                if j > 1 or (dz == 0 and dy == 0):
                    continue
                gg, ff = at_zy(z + dz, y + dy)
                pltpu.make_async_remote_copy(
                    src_ref=slots_x.at[p, j, (y + dy) & 3, pl.ds(lo, hi - lo)],
                    dst_ref=tok.at[p, t, j * 4 + y, pl.ds(lo, hi - lo)],
                    send_sem=tsend.at[0],
                    recv_sem=trecv.at[p, j],
                    device_id=(gg, ff, t),
                    device_id_type=MESH,
                ).start()
        tok[p, t, y] = slots_x[p, 0, y]

    def near_copies(d):
        gg, ff = at_zy(z + 1 - 2 * d, y)
        return [
            pltpu.make_async_remote_copy(
                src_ref=src.at[d],
                dst_ref=dst.at[d],
                send_sem=nsend.at[d, i],
                recv_sem=nrecv.at[d, i],
                device_id=(gg, ff, t),
                device_id_type=MESH,
            )
            for i, (src, dst) in enumerate(((near_x, got_x), (near_m, got_m)))
        ]

    def pass_near(d):
        for cp in near_copies(d):
            cp.wait_recv()
        for p in range(2):
            number = (lax.broadcasted_iota(jnp.int32, (256, 256), 0) + p * 256).astype(F32)
            pick = (number == got_m[d, 0:1]) | (number == got_m[d, 1:2])
            rows = jnp.dot(jnp.where(pick, 1.0, 0.0).astype(BF), got_x[d], preferred_element_type=F32)
            spread[d, p] = rows.astype(BF).reshape(4, 64, 256)
            for dy in (2, 1, 3):
                gg, ff = at_zy(z, y + dy)
                pltpu.make_async_remote_copy(
                    src_ref=spread.at[d, p, (y + dy) & 3],
                    dst_ref=tok.at[p, t, (d + 2) * 4 + y],
                    send_sem=tsend.at[0],
                    recv_sem=trecv.at[p, 2],
                    device_id=(gg, ff, t),
                    device_id_type=MESH,
                ).start()
            tok[p, t, (d + 2) * 4 + y] = spread[d, p, y]

    def await_tokens(sems, p, part):
        ref = tok.at[p, t, pl.ds(0, (3, 4, 6)[part])]
        pltpu.make_async_copy(ref, ref, sems.at[p, part]).wait()

    def back(p, sem):
        return (ans, ansa, ansb)[sem]

    def send_back(p, plane, sem, lanes):
        for j, dz, lo, hi in PLANES:
            for dy in range(4):
                if j != plane or (dz == 0 and dy == 0):
                    continue
                gg, ff = at_zy(z - dz, y + dy)
                pltpu.make_async_remote_copy(
                    src_ref=outs.at[p, j * 4 + ((y + dy) & 3), pl.ds(lo, hi - lo), lanes],
                    dst_ref=back(p, sem).at[f, pl.ds(lo, hi - lo)],
                    send_sem=rsend.at[sem],
                    recv_sem=rrecv.at[sem],
                    device_id=(gg, ff, t),
                    device_id_type=MESH,
                ).start()
        if plane == 0:
            back(p, sem)[f] = outs[p, y, :, lanes]

    def await_back(sems, p, sem, lanes):
        part = outs.at[p, pl.ds(0, 15), :, lanes]
        pltpu.make_async_copy(part, part, sems.at[sem]).wait()

    def send_dx(p, h):
        def body(i, carry):
            tt = (t + i) & 7
            pltpu.make_async_remote_copy(
                src_ref=w_d.at[p, pl.ds(tt * 4, 4), pl.ds(32 * h, 32)],
                dst_ref=dx.at[p, h, t],
                send_sem=dsend.at[0],
                recv_sem=drecv.at[p, h],
                device_id=(g, f, tt),
                device_id_type=MESH,
            ).start()
            return carry

        lax.fori_loop(1, 8, body, 0)
        dx[p, h, t] = w_d[p, pl.ds(t * 4, 4), pl.ds(32 * h, 32)]

    def await_dx(sems, p, h):
        part = dx.at[p, h, pl.ds(0, 7)]
        pltpu.make_async_copy(part, part, sems.at[p, h]).wait()

    def hidden(p):
        for r in (2, 3, 0, 1):
            rows = jnp.concatenate([tok[p, tt, pl.ds(r * 4, 4)].reshape(256, 256) for tt in range(8)], axis=1)
            pre = jnp.dot(rows, w_gu[p][...].reshape(2048, 256), preferred_element_type=F32) * 2048 ** (-0.5)
            gate, up = pre[:, 0:128], pre[:, 128:256]
            value = gate / (1.0 + jnp.exp(-gate)) * up
            hid[p, t, pl.ds(r * 256, 256)] = value.astype(BF)
            if r == 3:
                own_left(HID0 + p, 2)
            elif r < 2:
                own_right(HID0 + p, r)
        own_right(HID0 + p, 2)
        own_left(HID0 + p, 0)
        own_left(HID0 + p, 1)
        own_other(HID0 + p)

    def expert_out(p, halves, sem, lanes):
        for r in (1, 2, 3, 0):
            rows = jnp.concatenate([hid[p, tt, pl.ds(r * 256, 256)] for tt in range(8)], axis=1)
            cols = jnp.concatenate(
                [
                    jnp.concatenate([dx[p, h, tt].reshape(128, 128) for tt in range(8)], axis=1)
                    for h in halves
                ],
                axis=0,
            )
            value = lax.dot_general(rows, cols, (((1,), (1,)), ((), ())), preferred_element_type=F32)
            value = (value * 1024 ** (-0.5)).astype(BF)
            outs[p, pl.ds(r * 4, 4), :, lanes] = value.reshape(4, 64, 128 * len(halves))
            send_back(p, r, sem, lanes)

    def blend(p, sem, lanes):
        for r in range(2):
            rows = pl.ds(r * 256, 256)
            values = back(p, sem)[...].reshape(1024, lanes.size)
            part = jnp.dot((hi0, hi1)[p][rows], values, preferred_element_type=F32)
            part += jnp.dot((lo0, lo1)[p][rows], values, preferred_element_type=F32)
            if p == 0:
                acc[rows] = part
            else:
                acc[rows, lanes] += part

    whole = pl.ds(0, 256)
    low, high = pl.ds(0, 128), pl.ds(128, 128)
    all_rows = pl.ds(0, 64)
    rows_a, rows_b = pl.ds(0, 32), pl.ds(32, 32)

    loads[0].wait()
    row_i = lax.broadcasted_iota(jnp.int32, (512, 512), 0)
    col_i = lax.broadcasted_iota(jnp.int32, (512, 512), 1)
    diag = col_i == row_i

    def column(row):
        return jnp.sum(jnp.where(diag, row, 0.0), axis=1, keepdims=True)

    experts = lax.broadcasted_iota(jnp.int32, (32, 512), 0)
    hit0 = jnp.where(routes_ref[0:1] == experts, 1.0, 0.0)
    hit1 = jnp.where(routes_ref[1:2] == experts, 1.0, 0.0)
    before = jnp.where(row_i < col_i, 1.0, 0.0).astype(BF)
    rank0 = jnp.dot(hit0.astype(BF), before, preferred_element_type=F32)
    rank1 = jnp.dot(hit1.astype(BF), before, preferred_element_type=F32) + jnp.sum(hit0, axis=1, keepdims=True)
    place = ((experts >> 1) * 64 + (experts & 1) * 1024).astype(F32)
    slot0_row = jnp.sum((rank0 + place) * hit0, axis=0, keepdims=True)
    slot1_row = jnp.sum((rank1 + place) * hit1, axis=0, keepdims=True)

    loads[1].wait()
    wide = prompt_v[...].astype(F32)
    scale = lax.rsqrt(jnp.sum(wide * wide, axis=1, keepdims=True) * (1.0 / 2048) + EPS)
    mine = prompt_v[:, pl.ds(pl.multiple_of(t * 256, 256), 256)].astype(F32)
    normed = (mine * scale).astype(BF)

    def group_of(dz):
        return ((z + dz) & 3).astype(F32)

    numbers = lax.broadcasted_iota(jnp.int32, (256, 512), 0).astype(F32)

    def pick_slots(p):
        for j in range(2):
            number = numbers + (group_of(2 * j) * 256.0 + p * 1024.0)
            pick = jnp.where((number == slot0_row) | (number == slot1_row), 1.0, 0.0).astype(BF)
            rows = jnp.dot(pick, normed, preferred_element_type=F32).astype(BF)
            slots_x[p, j] = rows.reshape(4, 64, 256)

    def along(values, hit):
        return jnp.sum(values.astype(F32) * hit, axis=0, keepdims=True)

    group_row = along(experts >> 3, hit0)
    groups = lax.broadcasted_iota(jnp.int32, (8, 512), 0).astype(F32)
    group_hit = jnp.where(groups == group_row, 1.0, 0.0)
    group_rank = jnp.dot(group_hit.astype(BF), before, preferred_element_type=F32)
    number_row = along(group_rank, group_hit) + group_row * 256.0
    facts = (
        along(experts & 1, hit0),
        along((experts >> 1) & 3, hit0),
        along(rank0, hit0),
        along(experts & 1, hit1),
        along((experts >> 1) & 3, hit1),
        along(rank1, hit1),
        jnp.ones((1, 512), F32),
        jnp.zeros((1, 512), F32),
    )
    facts = jnp.concatenate(facts, axis=0).astype(BF)
    for d in range(2):
        pick = jnp.where(numbers + group_of(1 - 2 * d) * 256.0 == number_row, 1.0, 0.0).astype(BF)
        near_x[d] = jnp.dot(pick, normed, preferred_element_type=F32).astype(BF)
        m = lax.dot_general(facts, pick, (((1,), (1,)), ((), ())), preferred_element_type=F32)
        first = m[0:1] * 256.0 + m[1:2] * 64.0 + m[2:3] + (m[6:7] - 1.0)
        second = m[3:4] * 256.0 + m[4:5] * 64.0 + m[5:6] + (m[6:7] - 1.0)
        near_m[d] = jnp.concatenate([first, second, m[2:8]], axis=0)
    pick_slots(0)
    pick_slots(1)
    loads[4].wait()
    round_d(0)
    pl.semaphore_wait(barrier, 38)
    for d in range(2):
        for cp in near_copies(d):
            cp.start()
    send_tokens(0)
    send_tokens(1)
    loads[2].wait()
    loads[3].wait()
    loads[5].wait()
    eye = lax.broadcasted_iota(jnp.int32, (64, 64), 0) == lax.broadcasted_iota(jnp.int32, (64, 64), 1)
    gain = jnp.sum(jnp.where(eye, gain_ref[...], 0.0), axis=1, keepdims=True)
    round_gu(0, gain)
    send_w(stage_gu.at[0], w_gu0, 2, all_rows, 1, 8, 4)
    round_gu(1, gain)
    for p in range(2):
        await_tokens(trecv, p, 0)
        own_right(p, 0)
        own_left(p, 0)
    pass_near(0)
    pass_near(1)
    send_w_other(stage_gu.at[0], w_gu0, 2)
    send_w(stage_gu.at[1], w_gu1, 3, all_rows)
    send_w(stage_d.at[0], w_d.at[0], 0, all_rows)
    round_d(1)
    send_w(stage_d.at[1], w_d.at[1], 1, rows_a)
    send_w(stage_d.at[1], w_d.at[1], 4, rows_b)
    for p in range(2):
        await_tokens(trecv, p, 1)
        own_right(p, 1)
        own_left(p, 1)
    relay_right(TOK0, 0)
    await_tokens(trecv, 0, 2)
    own_left(TOK0, 2)
    own_right(TOK0, 2)
    own_other(TOK0)
    relay_right(TOK1, 0)
    await_tokens(trecv, 1, 2)
    own_left(TOK1, 2)
    own_right(TOK1, 2)
    own_other(TOK1)
    relay_right(TOK0, 1)
    loads[6].wait()
    slot0 = column(slot0_row)
    slot1 = column(slot1_row)
    rw0 = column(rw_ref[0:1])
    rw1 = column(rw_ref[1:2])
    for p in range(2):
        for r in range(4):
            cols = pl.ds(r * 256, 256)
            number = (lax.broadcasted_iota(jnp.int32, (512, 256), 1) + (p * 1024 + r * 256)).astype(F32)
            weight = jnp.where(number == slot0, rw0, jnp.where(number == slot1, rw1, 0.0))
            upper = weight.astype(BF)
            (hi0, hi1)[p][:, cols] = upper
            (lo0, lo1)[p][:, cols] = (weight - upper.astype(F32)).astype(BF)
    relay_right(TOK1, 1)
    relay_left(TOK0)
    ag_pass(TOK0)
    relay_left(TOK1)
    ag_pass(TOK1)
    ag_far(TOK0)
    ag_end(TOK0)
    await_w(wrecv, w_gu0, 2, all_rows)
    hidden(0)
    ag_far(TOK1)
    ag_end(TOK1)
    relay_left(HID0)
    relay_right(HID0, 0)
    relay_right(HID0, 1)
    ag_pass(HID0)
    ag_far(HID0)
    ag_end(HID0)
    await_w(wrecv, w_gu1, 3, all_rows)
    hidden(1)
    relay_left(HID1)
    relay_right(HID1, 0)
    relay_right(HID1, 1)
    ag_pass(HID1)
    await_w(wrecv, w_d.at[0], 0, all_rows)
    send_dx(0, 0)
    send_dx(0, 1)
    ag_far(HID1)
    ag_end(HID1)
    await_dx(drecv, 0, 0)
    await_w(wrecv, w_d.at[1], 1, rows_a)
    send_dx(1, 0)
    await_dx(drecv, 0, 1)
    expert_out(0, (0, 1), 0, whole)
    await_w(wrecv, w_d.at[1], 4, rows_b)
    send_dx(1, 1)
    await_dx(drecv, 1, 0)
    expert_out(1, (0,), 1, low)
    await_dx(drecv, 1, 1)
    expert_out(1, (1,), 2, high)
    for kind in range(4):
        ag_drain(kind)
    for d in range(2):
        for cp in near_copies(d):
            cp.wait_send()
    for ref, sem in ((tok.at[0, pl.ds(0, 2), pl.ds(0, 13)], tsend), (dx.at[:, :, pl.ds(0, 7)], dsend)):
        pltpu.make_async_copy(ref, ref, sem.at[0]).wait()
    await_w(wsend, w_d.at[0], 0, all_rows)
    await_w(wsend, w_d.at[1], 1, rows_a)
    await_w(wsend, w_gu0, 2, all_rows)
    await_w(wsend, w_gu1, 3, all_rows)
    await_w(wsend, w_d.at[1], 4, rows_b)
    await_back(rrecv, 0, 0, whole)
    blend(0, 0, whole)
    await_back(rsend, 0, 0, whole)
    await_back(rrecv, 1, 1, low)
    blend(1, 1, low)
    await_back(rsend, 1, 1, low)
    await_back(rsend, 1, 2, high)
    await_back(rrecv, 1, 2, high)


def copy_out(
    w_gu0,
    w_gu1,
    w_d,
    hi1,
    lo1,
    acc,
    ansb,
    gate_out,
    up_out,
    down_out,
    blend_out,
    blend_v,
    sem,
):
    copies = [
        pltpu.make_async_copy(w_gu0.at[:, :, pl.ds(0, 128)], gate_out.at[0], sem.at[0]),
        pltpu.make_async_copy(w_gu1.at[:, :, pl.ds(0, 128)], gate_out.at[1], sem.at[1]),
        pltpu.make_async_copy(w_gu0.at[:, :, pl.ds(128, 128)], up_out.at[0], sem.at[2]),
        pltpu.make_async_copy(w_gu1.at[:, :, pl.ds(128, 128)], up_out.at[1], sem.at[3]),
        pltpu.make_async_copy(w_d, down_out, sem.at[4]),
        pltpu.make_async_copy(blend_v, blend_out, sem.at[5]),
    ]
    for cp in copies[:5]:
        cp.start()
    a = lax.broadcasted_iota(jnp.int32, (256, 256), 0)
    b = lax.broadcasted_iota(jnp.int32, (256, 256), 1)
    goes = a == ((b >> 5) & 1) * 128 + (b >> 6) * 32 + (b & 31)
    to_place = jnp.where(goes, 1.0, 0.0).astype(BF)
    values = ansb[...].reshape(1024, 128)
    part = jnp.dot(hi1[...], values, preferred_element_type=F32)
    part += jnp.dot(lo1[...], values, preferred_element_type=F32)
    total = jnp.concatenate([acc[:, 0:128], acc[:, 128:256] + part], axis=1).astype(BF)
    blend_v[...] = jnp.dot(total, to_place, preferred_element_type=F32).astype(BF)
    copies[5].start()
    for cp in copies:
        cp.wait()


def per_device(prompt, norm_gain, gate_master, up_master, down_master, routes, route_weights):
    hbm = pl.BlockSpec(memory_space=pltpu.HBM)
    vmem = pl.BlockSpec(memory_space=pltpu.VMEM)
    ready = jax.ShapeDtypeStruct((2, 32, 64, 128), BF)
    both = jax.ShapeDtypeStruct((32, 64, 256), BF)
    block = jax.ShapeDtypeStruct((512, 256), BF)
    select = jax.ShapeDtypeStruct((512, 1024), BF)
    total = jax.ShapeDtypeStruct((512, 256), F32)
    part = jax.ShapeDtypeStruct((16, 64, 128), BF)
    dma = pltpu.SemaphoreType.DMA
    split = lambda a: a.reshape(16, 2, 64, 128)
    passed = pl.pallas_call(
        kernel,
        out_shape=(both, both, ready, select, select, total, part),
        in_specs=[hbm] * 7,
        out_specs=(vmem,) * 7,
        scratch_shapes=[
            pltpu.VMEM((1, 64), F32),
            pltpu.VMEM((2, 512), jnp.int32),
            pltpu.VMEM((2, 512), F32),
            pltpu.VMEM((512, 2048), BF),
            pltpu.VMEM((16, 2, 64, 128), F32),
            pltpu.VMEM((16, 2, 64, 128), F32),
            pltpu.VMEM((16, 2, 64, 128), F32),
            pltpu.VMEM((2, 16, 64, 256), BF),
            pltpu.VMEM((2, 16, 64, 128), BF),
            pltpu.VMEM((2, 2, 4, 64, 256), BF),
            pltpu.VMEM((2, 256, 256), BF),
            pltpu.VMEM((2, 8, 256), F32),
            pltpu.VMEM((2, 256, 256), BF),
            pltpu.VMEM((2, 8, 256), F32),
            pltpu.VMEM((2, 2, 4, 64, 256), BF),
            pltpu.VMEM((2, 8, 16, 64, 256), BF),
            pltpu.VMEM((2, 8, 1024, 128), BF),
            pltpu.VMEM((2, 2, 8, 4, 32, 128), BF),
            pltpu.VMEM((2, 16, 64, 256), BF),
            pltpu.VMEM((16, 64, 256), BF),
            pltpu.VMEM((16, 64, 128), BF),
            pltpu.VMEM((512, 1024), BF),
            pltpu.VMEM((512, 1024), BF),
            dma((7,)),
            dma((5,)),
            dma((5,)),
            dma((1,)),
            dma((2, 3)),
            dma((2, 2)),
            dma((2, 2)),
            dma((4,)),
            dma((4, 8)),
            dma((1,)),
            dma((2, 2)),
            dma((3,)),
            dma((3,)),
        ],
        compiler_params=pltpu.CompilerParams(
            collective_id=0, has_side_effects=True, vmem_limit_bytes=48 * 2**20
        ),
    )(
        *[
            pltpu.with_memory_space_constraint(a, pltpu.HBM)
            for a in (
                prompt,
                norm_gain.reshape(1, 64),
                split(gate_master),
                split(up_master),
                split(down_master),
                routes.T,
                route_weights.T,
            )
        ]
    )
    gate, up, down, out = pl.pallas_call(
        copy_out,
        out_shape=(ready, ready, ready, block),
        in_specs=[vmem] * 7,
        out_specs=(hbm,) * 4,
        scratch_shapes=[pltpu.VMEM((512, 256), BF), dma((6,))],
        compiler_params=pltpu.CompilerParams(vmem_limit_bytes=16 * 2**20),
    )(*passed)
    flat = lambda a: a.reshape(2, 2048, 128)
    return flat(gate), flat(up), flat(down), out


def solution(mesh):
    in_specs = (
        P(("gr", "fs"), None),
        P(("gr", "fs")),
        P(None, ("gr", "fs"), "tp"),
        P(None, ("gr", "fs"), "tp"),
        P(None, ("gr", "fs"), "tp"),
        P(("gr", "fs"), None),
        P(("gr", "fs"), None),
    )
    out_specs = (
        P("fs", None, "tp"),
        P("fs", None, "tp"),
        P("fs", None, "tp"),
        P(("gr", "fs"), "tp"),
    )
    return jax.shard_map(
        per_device, mesh=mesh, in_specs=in_specs, out_specs=out_specs, check_vma=False
    )
```

```python
import jax
import jax.numpy as jnp
from jax import lax
from jax.experimental import pallas as pl
from jax.experimental.pallas import tpu as pltpu
from jax.sharding import PartitionSpec as P

MESH = pl.DeviceIdType.MESH
EPS = 1e-06
BF = jnp.bfloat16
F32 = jnp.float32

PLANES = ((0, 0, 0, 64), (1, 2, 0, 32), (1, -2, 32, 64), (2, 1, 0, 64), (3, -1, 0, 64))
TOK0, TOK1, HID0, HID1 = 0, 1, 2, 3
TO_R, TO_L, TO_L2, FAR_R, FAR_L, ACROSS = 0, 3, 4, 5, 6, 7
PIECES = ((0, 4), (4, 4), (8, 8), (0, 8), (0, 16))
FIRST, WHOLE = 3, 4


def kernel(
    prompt_hbm,
    gain_hbm,
    gate_hbm,
    up_hbm,
    down_hbm,
    routes_hbm,
    rw_hbm,
    w_gu0,
    w_gu1,
    w_d,
    hi1,
    lo1,
    acc,
    ansb,
    gain_ref,
    routes_ref,
    rw_ref,
    prompt_v,
    gate_v,
    up_v,
    down_v,
    stage_gu,
    stage_d,
    slots_x,
    near_x,
    near_m,
    got_x,
    got_m,
    spread,
    tok,
    hid,
    dx,
    outs,
    ans,
    ansa,
    hi0,
    lo0,
    load_sem,
    wsend,
    wrecv,
    tsend,
    trecv,
    nsend,
    nrecv,
    asend,
    arecv,
    dsend,
    drecv,
    rsend,
    rrecv,
):
    w_gu = (w_gu0, w_gu1)
    g = lax.axis_index("gr")
    f = lax.axis_index("fs")
    t = lax.axis_index("tp")
    me = g * 16 + f
    z = g * 4 + (f >> 2)
    y = f & 3
    x = t >> 1
    c = t & 1

    def at_zy(zz, yy):
        zz = (zz + 8) & 7
        yy = (yy + 4) & 3
        return zz >> 2, ((zz & 3) << 2) + yy

    right = (g, f, ((x + 1) & 3) * 2 + c)
    left = (g, f, ((x + 3) & 3) * 2 + c)
    other = (g, f, x * 2 + 1 - c)
    t_l = ((x + 3) & 3) * 2 + c
    t_r = ((x + 1) & 3) * 2 + c
    t_f = ((x + 2) & 3) * 2 + c

    barrier = pltpu.get_barrier_semaphore()

    def greet_zy(i, carry):
        gg, ff = at_zy(z + (i >> 2), y + (i & 3))
        pl.semaphore_signal(barrier, inc=1, device_id=(gg, ff, t), device_id_type=MESH)
        return carry

    lax.fori_loop(1, 32, greet_zy, 0)

    def greet_tp(i, carry):
        pl.semaphore_signal(barrier, inc=1, device_id=(g, f, (t + i) & 7), device_id_type=MESH)
        return carry

    lax.fori_loop(1, 8, greet_tp, 0)

    loads = [
        pltpu.make_async_copy(routes_hbm, routes_ref, load_sem.at[0]),
        pltpu.make_async_copy(prompt_hbm, prompt_v, load_sem.at[1]),
        pltpu.make_async_copy(gate_hbm, gate_v, load_sem.at[2]),
        pltpu.make_async_copy(up_hbm, up_v, load_sem.at[3]),
        pltpu.make_async_copy(down_hbm, down_v, load_sem.at[4]),
        pltpu.make_async_copy(gain_hbm, gain_ref, load_sem.at[5]),
        pltpu.make_async_copy(rw_hbm, rw_ref, load_sem.at[6]),
    ]
    for ld in loads:
        ld.start()

    def round_d(p):
        def body(i, carry):
            stage_d[p, i] = down_v[i, p].astype(BF)
            return carry

        lax.fori_loop(0, 16, body, 0)
        w_d[p, me] = stage_d[p, f]

    def round_gu(p, gain):
        def body(i, carry):
            stage_gu[p, i, :, 0:128] = (gain * gate_v[i, p]).astype(BF)
            stage_gu[p, i, :, 128:256] = (gain * up_v[i, p]).astype(BF)
            return carry

        lax.fori_loop(0, 16, body, 0)
        w_gu[p][me] = stage_gu[p, f]

    def send_w(stage, dest, sem, rows, first=1, last=32, step=1):
        def body(n, carry):
            i = n * step
            gg, ff = at_zy(z + (i >> 2), y + (i & 3))
            pltpu.make_async_remote_copy(
                src_ref=stage.at[ff, rows],
                dst_ref=dest.at[me, rows],
                send_sem=wsend.at[sem],
                recv_sem=wrecv.at[sem],
                device_id=(gg, ff, t),
                device_id_type=MESH,
            ).start()
            return carry

        lax.fori_loop(first, last, body, 0)

    def send_w_other(stage, dest, sem):
        def body(n, carry):
            i = n + n // 3 + 1
            gg, ff = at_zy(z + (i >> 2), y + (i & 3))
            pltpu.make_async_remote_copy(
                src_ref=stage.at[ff],
                dst_ref=dest.at[me],
                send_sem=wsend.at[sem],
                recv_sem=wrecv.at[sem],
                device_id=(gg, ff, t),
                device_id_type=MESH,
            ).start()
            return carry

        lax.fori_loop(0, 24, body, 0)

    def await_w(sems, dest, sem, rows):
        part = dest.at[pl.ds(0, 31), rows]
        pltpu.make_async_copy(part, part, sems.at[sem]).wait()

    def copy_to(ref, sems, i, where):
        return pltpu.make_async_remote_copy(
            src_ref=ref,
            dst_ref=ref,
            send_sem=asend.at[sems],
            recv_sem=arecv.at[sems, i],
            device_id=where,
            device_id_type=MESH,
        )

    def piece(kind, tt, part):
        lo, size = PIECES[part]
        if kind < 2:
            return tok.at[kind, tt, pl.ds(lo, size)]
        return hid.at[kind - 2, tt, pl.ds(64 * lo, 64 * size)]

    def own_right(kind, part):
        copy_to(piece(kind, t, part), kind, TO_R + part, right).start()

    def own_left(kind, part):
        copy_to(piece(kind, t, part), kind, TO_L2 if part == 2 else TO_L, left).start()

    def own_other(kind):
        copy_to(piece(kind, t, WHOLE), kind, ACROSS, other).start()

    def relay_right(kind, part):
        copy_to(piece(kind, t_l, part), kind, TO_R + part, right).wait_recv()
        copy_to(piece(kind, t_l, part), kind, FAR_R, right).start()

    def relay_left(kind):
        copy_to(piece(kind, t_r, 2), kind, TO_L2, left).wait_recv()
        copy_to(piece(kind, t_r, 2), kind, FAR_L, left).start()

    def ag_pass(kind):
        copy_to(piece(kind, t_l, 2), kind, TO_R + 2, right).wait_recv()
        copy_to(piece(kind, t_l, WHOLE), kind, ACROSS, other).start()
        copy_to(piece(kind, t_r, FIRST), kind, TO_L, left).wait_recv()
        copy_to(piece(kind, t_r, WHOLE), kind, ACROSS, other).start()

    def ag_far(kind):
        copy_to(piece(kind, t_f, FIRST), kind, FAR_R, right).wait_recv()
        copy_to(piece(kind, t_f, FIRST), kind, ACROSS, other).start()
        copy_to(piece(kind, t_f, 2), kind, FAR_L, left).wait_recv()
        copy_to(piece(kind, t_f, 2), kind, ACROSS, other).start()

    def slices(kind, count):
        return (tok, tok, hid, hid)[kind].at[kind & 1, pl.ds(0, count)]

    def ag_end(kind):
        ref = slices(kind, 4)
        pltpu.make_async_copy(ref, ref, arecv.at[kind, ACROSS]).wait()

    def ag_drain(kind):
        ref = slices(kind, 7)
        pltpu.make_async_copy(ref, ref, asend.at[kind]).wait()

    def send_tokens(p):
        for j, dz, lo, hi in PLANES:
            for dy in range(4):
                if j > 1 or (dz == 0 and dy == 0):
                    continue
                gg, ff = at_zy(z + dz, y + dy)
                pltpu.make_async_remote_copy(
                    src_ref=slots_x.at[p, j, (y + dy) & 3, pl.ds(lo, hi - lo)],
                    dst_ref=tok.at[p, t, j * 4 + y, pl.ds(lo, hi - lo)],
                    send_sem=tsend.at[0],
                    recv_sem=trecv.at[p, j],
                    device_id=(gg, ff, t),
                    device_id_type=MESH,
                ).start()
        tok[p, t, y] = slots_x[p, 0, y]

    def near_copies(d):
        gg, ff = at_zy(z + 1 - 2 * d, y)
        return [
            pltpu.make_async_remote_copy(
                src_ref=src.at[d],
                dst_ref=dst.at[d],
                send_sem=nsend.at[d, i],
                recv_sem=nrecv.at[d, i],
                device_id=(gg, ff, t),
                device_id_type=MESH,
            )
            for i, (src, dst) in enumerate(((near_x, got_x), (near_m, got_m)))
        ]

    def pass_near(d):
        for cp in near_copies(d):
            cp.wait_recv()
        for p in range(2):
            number = (lax.broadcasted_iota(jnp.int32, (256, 256), 0) + p * 256).astype(F32)
            pick = (number == got_m[d, 0:1]) | (number == got_m[d, 1:2])
            rows = jnp.dot(jnp.where(pick, 1.0, 0.0).astype(BF), got_x[d], preferred_element_type=F32)
            spread[d, p] = rows.astype(BF).reshape(4, 64, 256)
            for dy in (2, 1, 3):
                gg, ff = at_zy(z, y + dy)
                pltpu.make_async_remote_copy(
                    src_ref=spread.at[d, p, (y + dy) & 3],
                    dst_ref=tok.at[p, t, (d + 2) * 4 + y],
                    send_sem=tsend.at[0],
                    recv_sem=trecv.at[p, 2],
                    device_id=(gg, ff, t),
                    device_id_type=MESH,
                ).start()
            tok[p, t, (d + 2) * 4 + y] = spread[d, p, y]

    def await_tokens(sems, p, part):
        ref = tok.at[p, t, pl.ds(0, (3, 4, 6)[part])]
        pltpu.make_async_copy(ref, ref, sems.at[p, part]).wait()

    def back(p, sem):
        return (ans, ansa, ansb)[sem]

    def send_back(p, plane, sem, lanes):
        for j, dz, lo, hi in PLANES:
            for dy in range(4):
                if j != plane or (dz == 0 and dy == 0):
                    continue
                gg, ff = at_zy(z - dz, y + dy)
                pltpu.make_async_remote_copy(
                    src_ref=outs.at[p, j * 4 + ((y + dy) & 3), pl.ds(lo, hi - lo), lanes],
                    dst_ref=back(p, sem).at[f, pl.ds(lo, hi - lo)],
                    send_sem=rsend.at[sem],
                    recv_sem=rrecv.at[sem],
                    device_id=(gg, ff, t),
                    device_id_type=MESH,
                ).start()
        if plane == 0:
            back(p, sem)[f] = outs[p, y, :, lanes]

    def await_back(sems, p, sem, lanes):
        part = outs.at[p, pl.ds(0, 15), :, lanes]
        pltpu.make_async_copy(part, part, sems.at[sem]).wait()

    def send_dx(p, h):
        def body(i, carry):
            tt = (t + i) & 7
            pltpu.make_async_remote_copy(
                src_ref=w_d.at[p, pl.ds(tt * 4, 4), pl.ds(32 * h, 32)],
                dst_ref=dx.at[p, h, t],
                send_sem=dsend.at[0],
                recv_sem=drecv.at[p, h],
                device_id=(g, f, tt),
                device_id_type=MESH,
            ).start()
            return carry

        lax.fori_loop(1, 8, body, 0)
        dx[p, h, t] = w_d[p, pl.ds(t * 4, 4), pl.ds(32 * h, 32)]

    def await_dx(sems, p, h):
        part = dx.at[p, h, pl.ds(0, 7)]
        pltpu.make_async_copy(part, part, sems.at[p, h]).wait()

    def hidden(p):
        for r in (2, 3, 0, 1):
            rows = jnp.concatenate([tok[p, tt, pl.ds(r * 4, 4)].reshape(256, 256) for tt in range(8)], axis=1)
            pre = jnp.dot(rows, w_gu[p][...].reshape(2048, 256), preferred_element_type=F32) * 2048 ** (-0.5)
            gate, up = pre[:, 0:128], pre[:, 128:256]
            value = gate / (1.0 + jnp.exp(-gate)) * up
            hid[p, t, pl.ds(r * 256, 256)] = value.astype(BF)
            if r == 3:
                own_left(HID0 + p, 2)
            elif r < 2:
                own_right(HID0 + p, r)
        own_right(HID0 + p, 2)
        own_left(HID0 + p, 0)
        own_left(HID0 + p, 1)
        own_other(HID0 + p)

    def expert_out(p, halves, sem, lanes):
        for r in (1, 2, 3, 0):
            rows = jnp.concatenate([hid[p, tt, pl.ds(r * 256, 256)] for tt in range(8)], axis=1)
            cols = jnp.concatenate(
                [
                    jnp.concatenate([dx[p, h, tt].reshape(128, 128) for tt in range(8)], axis=1)
                    for h in halves
                ],
                axis=0,
            )
            value = lax.dot_general(rows, cols, (((1,), (1,)), ((), ())), preferred_element_type=F32)
            value = (value * 1024 ** (-0.5)).astype(BF)
            outs[p, pl.ds(r * 4, 4), :, lanes] = value.reshape(4, 64, 128 * len(halves))
            send_back(p, r, sem, lanes)

    def blend(p, sem, lanes):
        for r in range(2):
            rows = pl.ds(r * 256, 256)
            values = back(p, sem)[...].reshape(1024, lanes.size)
            part = jnp.dot((hi0, hi1)[p][rows], values, preferred_element_type=F32)
            part += jnp.dot((lo0, lo1)[p][rows], values, preferred_element_type=F32)
            if p == 0:
                acc[rows] = part
            else:
                acc[rows, lanes] += part

    whole = pl.ds(0, 256)
    low, high = pl.ds(0, 128), pl.ds(128, 128)
    all_rows = pl.ds(0, 64)
    rows_a, rows_b = pl.ds(0, 32), pl.ds(32, 32)

    loads[0].wait()
    row_i = lax.broadcasted_iota(jnp.int32, (512, 512), 0)
    col_i = lax.broadcasted_iota(jnp.int32, (512, 512), 1)
    diag = col_i == row_i

    def column(row):
        return jnp.sum(jnp.where(diag, row, 0.0), axis=1, keepdims=True)

    experts = lax.broadcasted_iota(jnp.int32, (32, 512), 0)
    hit0 = jnp.where(routes_ref[0:1] == experts, 1.0, 0.0)
    hit1 = jnp.where(routes_ref[1:2] == experts, 1.0, 0.0)
    before = jnp.where(row_i < col_i, 1.0, 0.0).astype(BF)
    rank0 = jnp.dot(hit0.astype(BF), before, preferred_element_type=F32)
    rank1 = jnp.dot(hit1.astype(BF), before, preferred_element_type=F32) + jnp.sum(hit0, axis=1, keepdims=True)
    place = ((experts >> 1) * 64 + (experts & 1) * 1024).astype(F32)
    slot0_row = jnp.sum((rank0 + place) * hit0, axis=0, keepdims=True)
    slot1_row = jnp.sum((rank1 + place) * hit1, axis=0, keepdims=True)

    loads[1].wait()
    wide = prompt_v[...].astype(F32)
    scale = lax.rsqrt(jnp.sum(wide * wide, axis=1, keepdims=True) * (1.0 / 2048) + EPS)
    mine = prompt_v[:, pl.ds(pl.multiple_of(t * 256, 256), 256)].astype(F32)
    normed = (mine * scale).astype(BF)

    def group_of(dz):
        return ((z + dz) & 3).astype(F32)

    numbers = lax.broadcasted_iota(jnp.int32, (256, 512), 0).astype(F32)

    def pick_slots(p):
        for j in range(2):
            number = numbers + (group_of(2 * j) * 256.0 + p * 1024.0)
            pick = jnp.where((number == slot0_row) | (number == slot1_row), 1.0, 0.0).astype(BF)
            rows = jnp.dot(pick, normed, preferred_element_type=F32).astype(BF)
            slots_x[p, j] = rows.reshape(4, 64, 256)

    def along(values, hit):
        return jnp.sum(values.astype(F32) * hit, axis=0, keepdims=True)

    group_row = along(experts >> 3, hit0)
    groups = lax.broadcasted_iota(jnp.int32, (8, 512), 0).astype(F32)
    group_hit = jnp.where(groups == group_row, 1.0, 0.0)
    group_rank = jnp.dot(group_hit.astype(BF), before, preferred_element_type=F32)
    number_row = along(group_rank, group_hit) + group_row * 256.0
    facts = (
        along(experts & 1, hit0),
        along((experts >> 1) & 3, hit0),
        along(rank0, hit0),
        along(experts & 1, hit1),
        along((experts >> 1) & 3, hit1),
        along(rank1, hit1),
        jnp.ones((1, 512), F32),
        jnp.zeros((1, 512), F32),
    )
    facts = jnp.concatenate(facts, axis=0).astype(BF)
    for d in range(2):
        pick = jnp.where(numbers + group_of(1 - 2 * d) * 256.0 == number_row, 1.0, 0.0).astype(BF)
        near_x[d] = jnp.dot(pick, normed, preferred_element_type=F32).astype(BF)
        m = lax.dot_general(facts, pick, (((1,), (1,)), ((), ())), preferred_element_type=F32)
        first = m[0:1] * 256.0 + m[1:2] * 64.0 + m[2:3] + (m[6:7] - 1.0)
        second = m[3:4] * 256.0 + m[4:5] * 64.0 + m[5:6] + (m[6:7] - 1.0)
        near_m[d] = jnp.concatenate([first, second, m[2:8]], axis=0)
    pick_slots(0)
    pick_slots(1)
    loads[4].wait()
    round_d(0)
    pl.semaphore_wait(barrier, 38)
    for d in range(2):
        for cp in near_copies(d):
            cp.start()
    send_tokens(0)
    send_tokens(1)
    loads[2].wait()
    loads[3].wait()
    loads[5].wait()
    eye = lax.broadcasted_iota(jnp.int32, (64, 64), 0) == lax.broadcasted_iota(jnp.int32, (64, 64), 1)
    gain = jnp.sum(jnp.where(eye, gain_ref[...], 0.0), axis=1, keepdims=True)
    round_gu(0, gain)
    send_w(stage_gu.at[0], w_gu0, 2, all_rows, 1, 8, 4)
    round_gu(1, gain)
    for p in range(2):
        await_tokens(trecv, p, 0)
        own_right(p, 0)
        own_left(p, 0)
    pass_near(0)
    pass_near(1)
    send_w_other(stage_gu.at[0], w_gu0, 2)
    send_w(stage_gu.at[1], w_gu1, 3, all_rows)
    send_w(stage_d.at[0], w_d.at[0], 0, all_rows)
    round_d(1)
    send_w(stage_d.at[1], w_d.at[1], 1, rows_a)
    send_w(stage_d.at[1], w_d.at[1], 4, rows_b)
    for p in range(2):
        await_tokens(trecv, p, 1)
        own_right(p, 1)
        own_left(p, 1)
    relay_right(TOK0, 0)
    await_tokens(trecv, 0, 2)
    own_left(TOK0, 2)
    own_right(TOK0, 2)
    own_other(TOK0)
    relay_right(TOK1, 0)
    await_tokens(trecv, 1, 2)
    own_left(TOK1, 2)
    own_right(TOK1, 2)
    own_other(TOK1)
    relay_right(TOK0, 1)
    loads[6].wait()
    slot0 = column(slot0_row)
    slot1 = column(slot1_row)
    rw0 = column(rw_ref[0:1])
    rw1 = column(rw_ref[1:2])
    for p in range(2):
        for r in range(4):
            cols = pl.ds(r * 256, 256)
            number = (lax.broadcasted_iota(jnp.int32, (512, 256), 1) + (p * 1024 + r * 256)).astype(F32)
            weight = jnp.where(number == slot0, rw0, jnp.where(number == slot1, rw1, 0.0))
            upper = weight.astype(BF)
            (hi0, hi1)[p][:, cols] = upper
            (lo0, lo1)[p][:, cols] = (weight - upper.astype(F32)).astype(BF)
    relay_right(TOK1, 1)
    relay_left(TOK0)
    ag_pass(TOK0)
    relay_left(TOK1)
    ag_pass(TOK1)
    ag_far(TOK0)
    ag_end(TOK0)
    await_w(wrecv, w_gu0, 2, all_rows)
    hidden(0)
    ag_far(TOK1)
    ag_end(TOK1)
    relay_left(HID0)
    relay_right(HID0, 0)
    relay_right(HID0, 1)
    ag_pass(HID0)
    ag_far(HID0)
    ag_end(HID0)
    await_w(wrecv, w_gu1, 3, all_rows)
    hidden(1)
    relay_left(HID1)
    relay_right(HID1, 0)
    relay_right(HID1, 1)
    ag_pass(HID1)
    await_w(wrecv, w_d.at[0], 0, all_rows)
    send_dx(0, 0)
    send_dx(0, 1)
    ag_far(HID1)
    ag_end(HID1)
    await_dx(drecv, 0, 0)
    await_w(wrecv, w_d.at[1], 1, rows_a)
    send_dx(1, 0)
    await_dx(drecv, 0, 1)
    expert_out(0, (0, 1), 0, whole)
    await_w(wrecv, w_d.at[1], 4, rows_b)
    send_dx(1, 1)
    await_dx(drecv, 1, 0)
    expert_out(1, (0,), 1, low)
    await_dx(drecv, 1, 1)
    expert_out(1, (1,), 2, high)
    for kind in range(4):
        ag_drain(kind)
    for d in range(2):
        for cp in near_copies(d):
            cp.wait_send()
    for ref, sem in ((tok.at[0, pl.ds(0, 2), pl.ds(0, 13)], tsend), (dx.at[:, :, pl.ds(0, 7)], dsend)):
        pltpu.make_async_copy(ref, ref, sem.at[0]).wait()
    await_w(wsend, w_d.at[0], 0, all_rows)
    await_w(wsend, w_d.at[1], 1, rows_a)
    await_w(wsend, w_gu0, 2, all_rows)
    await_w(wsend, w_gu1, 3, all_rows)
    await_w(wsend, w_d.at[1], 4, rows_b)
    await_back(rrecv, 0, 0, whole)
    blend(0, 0, whole)
    await_back(rsend, 0, 0, whole)
    await_back(rrecv, 1, 1, low)
    blend(1, 1, low)
    await_back(rsend, 1, 1, low)
    await_back(rsend, 1, 2, high)
    await_back(rrecv, 1, 2, high)


def copy_out(
    w_gu0,
    w_gu1,
    w_d,
    hi1,
    lo1,
    acc,
    ansb,
    gate_out,
    up_out,
    down_out,
    blend_out,
    blend_v,
    sem,
):
    copies = [
        pltpu.make_async_copy(w_gu0.at[:, :, pl.ds(0, 128)], gate_out.at[0], sem.at[0]),
        pltpu.make_async_copy(w_gu1.at[:, :, pl.ds(0, 128)], gate_out.at[1], sem.at[1]),
        pltpu.make_async_copy(w_gu0.at[:, :, pl.ds(128, 128)], up_out.at[0], sem.at[2]),
        pltpu.make_async_copy(w_gu1.at[:, :, pl.ds(128, 128)], up_out.at[1], sem.at[3]),
        pltpu.make_async_copy(w_d, down_out, sem.at[4]),
        pltpu.make_async_copy(blend_v.at[pl.ds(0, 256)], blend_out.at[pl.ds(0, 256)], sem.at[5]),
        pltpu.make_async_copy(blend_v.at[pl.ds(256, 256)], blend_out.at[pl.ds(256, 256)], sem.at[6]),
    ]
    for cp in copies[:5]:
        cp.start()
    a = lax.broadcasted_iota(jnp.int32, (256, 256), 0)
    b = lax.broadcasted_iota(jnp.int32, (256, 256), 1)
    goes = a == ((b >> 5) & 1) * 128 + (b >> 6) * 32 + (b & 31)
    to_place = jnp.where(goes, 1.0, 0.0).astype(BF)
    values = ansb[...].reshape(1024, 128)
    for r in range(2):
        rows = pl.ds(r * 256, 256)
        part = jnp.dot(hi1[rows], values, preferred_element_type=F32)
        part += jnp.dot(lo1[rows], values, preferred_element_type=F32)
        total = jnp.concatenate([acc[rows, 0:128], acc[rows, 128:256] + part], axis=1).astype(BF)
        blend_v[rows] = jnp.dot(total, to_place, preferred_element_type=F32).astype(BF)
        copies[5 + r].start()
    for cp in copies:
        cp.wait()


def per_device(prompt, norm_gain, gate_master, up_master, down_master, routes, route_weights):
    hbm = pl.BlockSpec(memory_space=pltpu.HBM)
    vmem = pl.BlockSpec(memory_space=pltpu.VMEM)
    ready = jax.ShapeDtypeStruct((2, 32, 64, 128), BF)
    both = jax.ShapeDtypeStruct((32, 64, 256), BF)
    block = jax.ShapeDtypeStruct((512, 256), BF)
    select = jax.ShapeDtypeStruct((512, 1024), BF)
    total = jax.ShapeDtypeStruct((512, 256), F32)
    part = jax.ShapeDtypeStruct((16, 64, 128), BF)
    dma = pltpu.SemaphoreType.DMA
    split = lambda a: a.reshape(16, 2, 64, 128)
    passed = pl.pallas_call(
        kernel,
        out_shape=(both, both, ready, select, select, total, part),
        in_specs=[hbm] * 7,
        out_specs=(vmem,) * 7,
        scratch_shapes=[
            pltpu.VMEM((1, 64), F32),
            pltpu.VMEM((2, 512), jnp.int32),
            pltpu.VMEM((2, 512), F32),
            pltpu.VMEM((512, 2048), BF),
            pltpu.VMEM((16, 2, 64, 128), F32),
            pltpu.VMEM((16, 2, 64, 128), F32),
            pltpu.VMEM((16, 2, 64, 128), F32),
            pltpu.VMEM((2, 16, 64, 256), BF),
            pltpu.VMEM((2, 16, 64, 128), BF),
            pltpu.VMEM((2, 2, 4, 64, 256), BF),
            pltpu.VMEM((2, 256, 256), BF),
            pltpu.VMEM((2, 8, 256), F32),
            pltpu.VMEM((2, 256, 256), BF),
            pltpu.VMEM((2, 8, 256), F32),
            pltpu.VMEM((2, 2, 4, 64, 256), BF),
            pltpu.VMEM((2, 8, 16, 64, 256), BF),
            pltpu.VMEM((2, 8, 1024, 128), BF),
            pltpu.VMEM((2, 2, 8, 4, 32, 128), BF),
            pltpu.VMEM((2, 16, 64, 256), BF),
            pltpu.VMEM((16, 64, 256), BF),
            pltpu.VMEM((16, 64, 128), BF),
            pltpu.VMEM((512, 1024), BF),
            pltpu.VMEM((512, 1024), BF),
            dma((7,)),
            dma((5,)),
            dma((5,)),
            dma((1,)),
            dma((2, 3)),
            dma((2, 2)),
            dma((2, 2)),
            dma((4,)),
            dma((4, 8)),
            dma((1,)),
            dma((2, 2)),
            dma((3,)),
            dma((3,)),
        ],
        compiler_params=pltpu.CompilerParams(
            collective_id=0, has_side_effects=True, vmem_limit_bytes=48 * 2**20
        ),
    )(
        *[
            pltpu.with_memory_space_constraint(a, pltpu.HBM)
            for a in (
                prompt,
                norm_gain.reshape(1, 64),
                split(gate_master),
                split(up_master),
                split(down_master),
                routes.T,
                route_weights.T,
            )
        ]
    )
    gate, up, down, out = pl.pallas_call(
        copy_out,
        out_shape=(ready, ready, ready, block),
        in_specs=[vmem] * 7,
        out_specs=(hbm,) * 4,
        scratch_shapes=[pltpu.VMEM((512, 256), BF), dma((7,))],
        compiler_params=pltpu.CompilerParams(vmem_limit_bytes=16 * 2**20),
    )(*passed)
    flat = lambda a: a.reshape(2, 2048, 128)
    return flat(gate), flat(up), flat(down), out


def solution(mesh):
    in_specs = (
        P(("gr", "fs"), None),
        P(("gr", "fs")),
        P(None, ("gr", "fs"), "tp"),
        P(None, ("gr", "fs"), "tp"),
        P(None, ("gr", "fs"), "tp"),
        P(("gr", "fs"), None),
        P(("gr", "fs"), None),
    )
    out_specs = (
        P("fs", None, "tp"),
        P("fs", None, "tp"),
        P("fs", None, "tp"),
        P(("gr", "fs"), "tp"),
    )
    return jax.shard_map(
        per_device, mesh=mesh, in_specs=in_specs, out_specs=out_specs, check_vma=False
    )
```
